128 devices in a mesh: sp: 16 (over z, y), tp: 8 (over x, core).
Axes of the slice: x: 4, y: 4, z: 4, core: 2. Of those that a mesh axis runs over, the one named last changes fastest.
Arguments:
- inputs: bfloat16 [16384, 4, 2048], P('sp'), may hold values from -6 to 6
- norm_gain: float32 [2048], replicated, may hold values from 0.1 to 1.9
- pool_proj: bfloat16 [2048, 1024], P(None, 'tp'), may hold values from -0.125 to 0.125
- pool_gate_proj: bfloat16 [2048, 1024], P(None, 'tp'), may hold values from -0.125 to 0.125
- pool_mix: bfloat16 [8, 128, 128], P('tp'), may hold values from -0.5 to 0.5
- query_proj: bfloat16 [2048, 1024], P(None, 'tp'), may hold values from -0.125 to 0.125
- key_proj: bfloat16 [2048, 512], P(None, 'tp'), may hold values from -0.125 to 0.125
- value_proj: bfloat16 [2048, 512], P(None, 'tp'), may hold values from -0.125 to 0.125
- attn_gate_proj: bfloat16 [2048, 1024], P(None, 'tp'), may hold values from -0.125 to 0.125
- query_gain: float32 [64], replicated, may hold values from 0.1 to 1.9
- key_gain: float32 [64], replicated, may hold values from 0.1 to 1.9
- sink_logit: float32 [16], P('tp'), may hold values from -12 to 240
- out_pool: bfloat16 [1024, 2048], P('sp'), may hold values from -0.125 to 0.125
- out_attn: bfloat16 [1024, 2048], P('sp'), may hold values from -0.125 to 0.125
Outputs:
- mixed_out: bfloat16 [16384, 4, 2048], P(('sp', 'tp'))
- log_weight_sum: float32 [16384, 4, 16], P('sp', None, 'tp')
The draws below stay inside these ranges and needn't reach their ends.
All inputs are finite; a program needn't handle non-finite values.
Results may differ from the reference program's by a relative error of at most 0.015.
Values may be sent and summed in bfloat16 or wider, within the bound.
No kernel may reach another device: no remote copies, remote signals or barrier semaphores. Data moves between devices by JAX's collectives and lax.ppermute only.
A program may use at most 192 MiB of HBM per device.

```python
import jax
import jax.numpy as jnp
from jax import lax

D = 2048
POOL_GROUPS = 8
GROUP_CH = 128
POOL_WIDTH = 1024
HEADS = 16
KV_HEADS = 8
HEAD_DIM = 64
GROUP_SIZE = 2
ATT_WIDTH = 1024
KV_WIDTH = 512
WINDOW = 128
SEQS = 4
SEQ_LEN = 16384


def draw_sink_logit(key, part):
    base = jnp.clip(2.0 * jax.random.normal(jax.random.fold_in(key, 1), (HEADS,), jnp.float32), -12.0, 12.0)
    return base


def shard_levels(stream_key, dims, shards, least, top_value):
    def one(dim, blocks):
        heights = jax.random.uniform(jax.random.fold_in(jax.random.fold_in(stream_key, 6), dim), (blocks,), jnp.float32, least / len(shards), top_value / len(shards))
        return jnp.repeat(jnp.exp(heights), dims[dim] // blocks).reshape((-1,) + (1,) * (len(dims) - dim - 1))

    factor_of = one(*shards[0])
    for cut in shards[1:]:
        factor_of = factor_of * one(*cut)
    return factor_of


def centred(stream_key, dims, width, reach, pieces=(), held_as=jnp.bfloat16):
    drawn = width * jax.random.normal(stream_key, dims, jnp.float32)
    if pieces:
        drawn = drawn * shard_levels(stream_key, dims, pieces, -0.22, 0.18)
    return jnp.clip(drawn, -reach, reach).astype(held_as)


def setup_inputs(seed: int = 0) -> dict:
    splits = jax.random.split(jax.random.key(seed), 15)
    inputs = centred(splits[0], (SEQ_LEN, SEQS, D), 1.0, 6.0, ((0, 16),))
    norm_gain = jnp.clip(1.0 + 0.18 * jax.random.normal(splits[1], (D,), jnp.float32), 0.1, 1.9)
    pool_proj = centred(splits[2], (D, POOL_WIDTH), D ** -0.5, 0.125, ((1, 8),))
    pool_gate_proj = centred(splits[3], (D, POOL_WIDTH), D ** -0.5, 0.125, ((1, 8),))
    pool_mix = centred(splits[4], (POOL_GROUPS, GROUP_CH, GROUP_CH), GROUP_CH ** -0.5, 0.5, ((0, 8),))
    query_proj = centred(splits[5], (D, ATT_WIDTH), D ** -0.5, 0.125, ((1, 8),))
    key_proj = centred(splits[6], (D, KV_WIDTH), D ** -0.5, 0.125, ((1, 8),))
    value_proj = centred(splits[7], (D, KV_WIDTH), D ** -0.5, 0.125, ((1, 8),))
    attn_gate_proj = centred(splits[8], (D, ATT_WIDTH), D ** -0.5, 0.125, ((1, 8),))
    query_gain = jnp.clip(1.0 + 0.18 * jax.random.normal(splits[9], (HEAD_DIM,), jnp.float32), 0.1, 1.9)
    key_gain = jnp.clip(1.0 + 0.18 * jax.random.normal(splits[10], (HEAD_DIM,), jnp.float32), 0.1, 1.9)
    sink_logit = draw_sink_logit(jax.random.fold_in(splits[14], 71), 0)
    out_pool = centred(splits[12], (POOL_WIDTH, D), (POOL_WIDTH + ATT_WIDTH) ** -0.5, 0.125, ((0, 16),))
    out_attn = centred(splits[13], (ATT_WIDTH, D), (POOL_WIDTH + ATT_WIDTH) ** -0.5, 0.125, ((0, 16),))
    return {"inputs": inputs, "norm_gain": norm_gain, "pool_proj": pool_proj, "pool_gate_proj": pool_gate_proj, "pool_mix": pool_mix, "query_proj": query_proj, "key_proj": key_proj, "value_proj": value_proj, "attn_gate_proj": attn_gate_proj, "query_gain": query_gain, "key_gain": key_gain, "sink_logit": sink_logit, "out_pool": out_pool, "out_attn": out_attn}


EPS = 1e-06
NEG = -1e+30

def stored(values):
    return lax.optimization_barrier(values.astype(jnp.bfloat16))

def reference(inputs, norm_gain, pool_proj, pool_gate_proj, pool_mix, query_proj, key_proj, value_proj, attn_gate_proj, query_gain, key_gain, sink_logit, out_pool, out_attn):
    seq_len = inputs.shape[0]
    flt = inputs.astype(jnp.float32)
    hidden = stored(flt * lax.rsqrt(lax.optimization_barrier(jnp.mean(flt * flt, axis=-1, keepdims=True)) + EPS) * norm_gain.astype(jnp.float32))

    def project(weight):
        return stored(jnp.dot(hidden, weight, preferred_element_type=jnp.float32))
    pool_in = project(pool_proj)
    pool_gate = project(pool_gate_proj)
    queries = project(query_proj)
    key_rows = project(key_proj)
    value_rows = project(value_proj)
    attn_gate = project(attn_gate_proj)
    pool_f = pool_in.astype(jnp.float32).reshape(seq_len, SEQS, POOL_GROUPS, GROUP_CH)
    prefix = jnp.concatenate([jnp.zeros((1, SEQS, POOL_GROUPS, GROUP_CH), jnp.float32), jnp.cumsum(pool_f, axis=0)], axis=0)
    positions = jnp.arange(seq_len, dtype=jnp.int32)
    means = []
    for group_id in range(POOL_GROUPS):
        half_width = 2 ** (group_id % 4)
        low_pos = jnp.clip(positions - half_width, 0, seq_len - 1)
        high_pos = jnp.clip(positions + half_width - 1, 0, seq_len - 1)
        window_sum = prefix[high_pos + 1, :, group_id] - prefix[low_pos, :, group_id]
        count_live = (high_pos - low_pos + 1).astype(jnp.float32)[:, None, None]
        means.append(window_sum / count_live)
    pooled = stored(jnp.stack(means, axis=2) - pool_f)
    pool_mixed = jnp.einsum('lsgc,gcd->lsgd', pooled.astype(jnp.float32), pool_mix.astype(jnp.float32))
    pool_mixed = pool_mixed.reshape(seq_len, SEQS, POOL_WIDTH)
    y_pool = stored(pool_mixed * jax.nn.silu(pool_gate.astype(jnp.float32)))

    def head_norm(values, heads, gain):
        flt_heads = values.astype(jnp.float32).reshape(seq_len, SEQS, heads, HEAD_DIM)
        return stored(flt_heads * lax.rsqrt(lax.optimization_barrier(jnp.mean(flt_heads * flt_heads, axis=-1, keepdims=True)) + EPS) * gain.astype(jnp.float32))
    normed_q = head_norm(queries, HEADS, query_gain).reshape(seq_len, SEQS, KV_HEADS, GROUP_SIZE, HEAD_DIM)
    normed_k = head_norm(key_rows, KV_HEADS, key_gain)
    value_heads = value_rows.reshape(seq_len, SEQS, KV_HEADS, HEAD_DIM)
    padding = ((WINDOW, WINDOW), (0, 0), (0, 0), (0, 0))
    key_pad = jnp.pad(normed_k, padding)
    value_pad = jnp.pad(value_heads, padding)
    slopes = (2.0 ** (-8.0 * jnp.arange(1, HEADS + 1, dtype=jnp.float32) / HEADS)).reshape(KV_HEADS, GROUP_SIZE)
    sink_vals = sink_logit.astype(jnp.float32).reshape(KV_HEADS, GROUP_SIZE)[None, :, :, None]

    def block(index):
        query_block = lax.dynamic_slice_in_dim(normed_q, index * WINDOW, WINDOW, 0)
        key_block = lax.dynamic_slice_in_dim(key_pad, index * WINDOW, 3 * WINDOW, 0)
        value_block = lax.dynamic_slice_in_dim(value_pad, index * WINDOW, 3 * WINDOW, 0)
        scores = jnp.einsum('qskgd,jskd->skgqj', query_block.astype(jnp.float32), key_block.astype(jnp.float32)) * HEAD_DIM ** (-0.5)
        query_pos = index * WINDOW + jnp.arange(WINDOW, dtype=jnp.int32)
        key_pos = index * WINDOW - WINDOW + jnp.arange(3 * WINDOW, dtype=jnp.int32)
        distance = jnp.abs(query_pos[:, None] - key_pos[None, :])
        usable = (distance <= WINDOW) & (key_pos >= 0)[None, :] & (key_pos < seq_len)[None, :]
        scores = scores - slopes[None, :, :, None, None] * distance.astype(jnp.float32)
        scores = jnp.where(usable, scores, NEG)
        row_top = jnp.maximum(lax.optimization_barrier(jnp.max(scores, axis=-1)), sink_vals)
        weights = jnp.exp(scores - row_top[..., None])
        weight_total = lax.optimization_barrier(jnp.sum(weights, axis=-1)) + jnp.exp(sink_vals - row_top)
        log_sum = row_top + jnp.log(weight_total)
        attended = jnp.einsum('skgqj,jskd->qskgd', stored(weights).astype(jnp.float32), value_block.astype(jnp.float32))
        attended = attended / jnp.transpose(weight_total, (3, 0, 1, 2))[..., None]
        return (attended.reshape(WINDOW, SEQS, ATT_WIDTH), jnp.transpose(log_sum, (3, 0, 1, 2)).reshape(WINDOW, SEQS, HEADS))
    attended, log_sums = lax.map(block, jnp.arange(seq_len // WINDOW, dtype=jnp.int32))
    attended = attended.reshape(seq_len, SEQS, ATT_WIDTH)
    log_weight_sum = log_sums.reshape(seq_len, SEQS, HEADS)
    y_attn = stored(attended * jax.nn.silu(attn_gate.astype(jnp.float32)))
    summed = jnp.dot(y_pool, out_pool, preferred_element_type=jnp.float32) + jnp.dot(y_attn, out_attn, preferred_element_type=jnp.float32)
    return (summed.astype(jnp.bfloat16), log_weight_sum)
```

```python
import math

import jax
import jax.numpy as jnp
from jax import lax
from jax.experimental import pallas as pl
from jax.experimental.pallas import tpu as pltpu
from jax.sharding import PartitionSpec as P

HEADS = 16
HEAD_DIM = 64
WINDOW = 128
REACH = 8
EPS = 1e-06
NEG = -1e30
LOG2E = math.log2(math.e)
F32 = jnp.float32
BF16 = jnp.bfloat16
BLOCK = 128


def row_scale(x):
    width = x.shape[1]
    acc = None
    for c in range(0, width, 128):
        part = x[:, c : c + 128].astype(F32)
        part = part * part
        acc = part if acc is None else acc + part
    total = jnp.sum(acc, axis=-1, keepdims=True)
    return lax.rsqrt(total * (1.0 / width) + EPS)


def silu(v):
    return v / (1.0 + jnp.exp(-v))


def edge_kernel(x_ref, w_ref, kv_ref, scr):
    half = x_ref.shape[0]
    x = x_ref.reshape(half * 4, x_ref.shape[2])[...]
    scale = row_scale(x)
    cols = jnp.dot(x, w_ref[...], preferred_element_type=F32) * scale
    scr[0] = cols[:, :128]
    scr[1] = cols[:, 128:]
    step = pl.program_id(0)
    for part in range(2):

        @pl.when(step % 2 == part)
        def _():
            for s in range(4):
                rows = scr[1, pl.ds(s, half, stride=4), :]
                kv_ref[0, s, part * half : (part + 1) * half, :] = rows.astype(BF16)

    @pl.when(step == 0)
    def _():
        for s in range(4):
            kv_ref[0, s, 128 : 128 + REACH, :] = scr[0, pl.ds(s, REACH, stride=4), :].astype(BF16)

    @pl.when(step == 3)
    def _():
        for s in range(4):
            tail = scr[0, pl.ds(s + 4 * (half - REACH), REACH, stride=4), :]
            kv_ref[0, s, 128 : 128 + REACH, :] = tail.astype(BF16)


def edges(x, w):
    half = 64
    last = x.shape[0] // half
    return pl.pallas_call(
        edge_kernel,
        grid=(4,),
        in_specs=[
            pl.BlockSpec((half, 4, x.shape[2]), lambda i: (i + (last - 4) * (i // 2), 0, 0)),
            pl.BlockSpec(w.shape, lambda i: (0, 0)),
        ],
        out_specs=pl.BlockSpec((1, 4, 136, 128), lambda i: (i // 2, 0, 0, 0)),
        out_shape=jax.ShapeDtypeStruct((2, 4, 136, 128), BF16),
        scratch_shapes=[pltpu.VMEM((2, half * 4, 128), F32)],
        compiler_params=pltpu.CompilerParams(dimension_semantics=("arbitrary",)),
        cost_estimate=pl.CostEstimate(flops=2 * 1024 * 2048 * 256, transcendentals=0, bytes_accessed=5 << 20),
        name="edge_rows",
    )(x, w)


def pool_kernel(ids, x_ref, w_ref, mix_ref, before_ref, after_ref, y_ref, pool, gate):
    step = pl.program_id(0)
    blocks = pl.num_programs(0) - 1
    rows = BLOCK * 4
    pad = 64
    total_rows = blocks * rows

    @pl.when(step == 0)
    def _():
        for s in range(4):
            pool[pl.ds(pad - 4 * REACH + s, REACH, stride=4), :] = before_ref[s, 128 : 128 + REACH, :].astype(F32)
            pool[pl.ds(pad + total_rows + s, REACH, stride=4), :] = after_ref[s, 128 : 128 + REACH, :].astype(F32)

    @pl.when(step < blocks)
    def _():
        x = x_ref.reshape(rows, x_ref.shape[2])[...]
        scale = row_scale(x)
        both = jnp.dot(x, w_ref[...], preferred_element_type=F32) * scale
        at = pl.multiple_of(step * rows, rows)
        pool[pl.ds(pad + at, rows), :] = both[:, :128]
        gate[pl.ds(at, rows), :] = both[:, 128:]

    @pl.when(step > 0)
    def _():
        at = pl.multiple_of((step - 1) * rows, rows)
        own = pool[pl.ds(pad + at, rows), :]
        sp, log_half, total_len = ids[0], ids[1], ids[2]
        position = sp * (blocks * BLOCK) + (step - 1) * BLOCK + lax.broadcasted_iota(jnp.int32, (rows, 128), 0) // 4

        def finish(half):
            window = pool[pl.ds(pad + at - 4 * REACH, rows + 8 * REACH), :]
            length = rows + 8 * REACH
            sums, width = window, 1
            while width < 2 * half:
                length -= 4 * width
                sums = sums[:length] + sums[4 * width : 4 * width + length]
                width *= 2
            begin = 4 * (REACH - half)
            window_sum = sums[begin : begin + rows]
            low = jnp.maximum(position - half, 0)
            high = jnp.minimum(position + half - 1, total_len - 1)
            count = (high - low + 1).astype(F32)
            pooled = (window_sum / count - own).astype(BF16)
            mixed = jnp.dot(pooled, mix_ref[0], preferred_element_type=F32)
            y_ref[0] = (mixed * silu(gate[pl.ds(at, rows), :])).astype(BF16)

        for k in range(4):

            @pl.when(log_half == k)
            def _(k=k):
                finish(2**k)


def pool_branch(ids, x, w, mix, before, after):
    length, _, width = x.shape
    blocks = length // BLOCK
    rows = BLOCK * 4
    return pl.pallas_call(
        pool_kernel,
        grid=(blocks + 1,),
        in_specs=[
            pl.BlockSpec(memory_space=pltpu.SMEM),
            pl.BlockSpec((BLOCK, 4, width), lambda i: (jnp.minimum(i, blocks - 1), 0, 0)),
            pl.BlockSpec(w.shape, lambda i: (0, 0)),
            pl.BlockSpec(mix.shape, lambda i: (0, 0, 0)),
            pl.BlockSpec(before.shape, lambda i: (0, 0, 0)),
            pl.BlockSpec(after.shape, lambda i: (0, 0, 0)),
        ],
        out_specs=pl.BlockSpec((1, rows, 128), lambda i: (jnp.maximum(i - 1, 0), 0, 0)),
        out_shape=jax.ShapeDtypeStruct((blocks, rows, 128), BF16),
        scratch_shapes=[
            pltpu.VMEM((length * 4 + 128, 128), F32),
            pltpu.VMEM((length * 4, 128), F32),
        ],
        compiler_params=pltpu.CompilerParams(dimension_semantics=("arbitrary",)),
        cost_estimate=pl.CostEstimate(flops=2 * 4096 * 2048 * 256, transcendentals=0, bytes_accessed=18 << 20),
        name="pool_branch",
    )(ids, x, w, mix, before, after)


def attn_kernel(ids, scal, x_ref, w_ref, gain_ref, before_ref, after_ref, y_ref, lse_ref, proj, qs, ks, vs, gate, bias, att):
    step = pl.program_id(0)
    blocks = pl.num_programs(0) - 1
    rows = BLOCK * 4
    lane = lax.broadcasted_iota(jnp.int32, (BLOCK, 128), 1)
    low_lanes = lane < HEAD_DIM

    @pl.when(step == 0)
    def _():
        query = lax.broadcasted_iota(jnp.int32, (BLOCK, 3 * BLOCK), 0)
        key = lax.broadcasted_iota(jnp.int32, (BLOCK, 3 * BLOCK), 1) - BLOCK
        distance = jnp.abs(query - key)
        for h in range(2):
            line = -scal[h] * distance.astype(F32) - scal[2 + h]
            bias[h * BLOCK : (h + 1) * BLOCK, :] = jnp.where(distance <= WINDOW, line, NEG)
        key_gain = gain_ref[:, 128:256]
        for side, ref in enumerate((before_ref, after_ref)):
            at = 0 if side == 0 else (blocks + 1) * BLOCK
            live = ids[3 + side].astype(F32)
            for s in range(4):
                kv = ref[s, 0:128, :].astype(F32)
                turned = pltpu.roll(kv, HEAD_DIM, 1)
                kk = jnp.where(low_lanes, kv, turned)
                vv = jnp.where(low_lanes, turned, kv)
                mean = jnp.sum(jnp.where(low_lanes, kv * kv, 0.0), axis=-1, keepdims=True) * (1.0 / HEAD_DIM)
                ks[s, at : at + BLOCK, :] = (kk * lax.rsqrt(mean + EPS) * key_gain).astype(BF16)
                vs[s, at : at + BLOCK, 0:128] = vv.astype(BF16)
                vs[s, at : at + BLOCK, 128:256] = jnp.full((BLOCK, 128), live, F32).astype(BF16)

    @pl.when(step < blocks)
    def _():
        x = x_ref.reshape(rows, x_ref.shape[2])[...]
        scale = row_scale(x)
        all_cols = jnp.dot(x, w_ref[...], preferred_element_type=F32) * scale
        qk = all_cols[:, :256]
        r = lax.broadcasted_iota(jnp.int32, (256, 256), 0) // HEAD_DIM
        c = lax.broadcasted_iota(jnp.int32, (256, 256), 1) // HEAD_DIM
        same = jnp.where(r == c, 1.0, 0.0).astype(BF16)
        squares = jnp.dot((qk * qk).astype(BF16), same, preferred_element_type=F32)
        normed = qk * lax.rsqrt(squares * (1.0 / HEAD_DIM) + EPS) * gain_ref[...]
        proj[0] = normed[:, :128]
        proj[1] = normed[:, 128:]
        proj[2] = all_cols[:, 256:384]
        at = pl.multiple_of(step * BLOCK, BLOCK)
        gate[pl.ds(pl.multiple_of(step * rows, rows), rows), :] = all_cols[:, 384:]
        for s in range(4):
            mine = pl.ds(s, BLOCK, stride=4)
            qs[s, pl.ds(at, BLOCK), :] = proj[0, mine, :].astype(BF16)
            ks[s, pl.ds(at + BLOCK, BLOCK), :] = proj[1, mine, :].astype(BF16)
            vs[s, pl.ds(at + BLOCK, BLOCK), 0:128] = proj[2, mine, :].astype(BF16)
            vs[s, pl.ds(at + BLOCK, BLOCK), 128:256] = jnp.ones((BLOCK, 128), BF16)

    @pl.when(step > 0)
    def _():
        at = pl.multiple_of((step - 1) * BLOCK, BLOCK)
        row_low = lax.broadcasted_iota(jnp.int32, (1, 128), 1) < HEAD_DIM
        sink_part = jnp.where(row_low, scal[4], scal[5])
        for s in range(4):
            q = qs[s, pl.ds(at, BLOCK), :]
            zero = jnp.zeros_like(q)
            two = jnp.concatenate([jnp.where(low_lanes, q, zero), jnp.where(low_lanes, zero, q)], axis=0)
            keys = ks[s, pl.ds(at, 3 * BLOCK), :]
            score = lax.dot_general(two, keys, (((1,), (1,)), ((), ())), preferred_element_type=F32)
            weight = jnp.exp2(score + bias[...]).astype(BF16)
            out = jnp.dot(weight, vs[s, pl.ds(at, 3 * BLOCK), :], preferred_element_type=F32)
            total = jnp.where(low_lanes, out[:BLOCK, 128:], out[BLOCK:, 128:]) + sink_part
            value = jnp.where(low_lanes, out[:BLOCK, :128], out[BLOCK:, :128])
            att[pl.ds(s, BLOCK, stride=4), :] = value / total
            turned = total.T
            lse_ref[s, 0:1, :] = jnp.log(turned[0:1, :]) + scal[6]
            lse_ref[s, 1:2, :] = jnp.log(turned[HEAD_DIM : HEAD_DIM + 1, :]) + scal[7]
        g = gate[pl.ds(pl.multiple_of((step - 1) * rows, rows), rows), :]
        y_ref[0] = (att[...] * silu(g)).astype(BF16)


def attn_branch(ids, scal, x, w, gain, before, after):
    length, _, width = x.shape
    blocks = length // BLOCK
    rows = BLOCK * 4
    return pl.pallas_call(
        attn_kernel,
        grid=(blocks + 1,),
        in_specs=[
            pl.BlockSpec(memory_space=pltpu.SMEM),
            pl.BlockSpec(memory_space=pltpu.SMEM),
            pl.BlockSpec((BLOCK, 4, width), lambda i: (jnp.minimum(i, blocks - 1), 0, 0)),
            pl.BlockSpec(w.shape, lambda i: (0, 0)),
            pl.BlockSpec(gain.shape, lambda i: (0, 0)),
            pl.BlockSpec(before.shape, lambda i: (0, 0, 0)),
            pl.BlockSpec(after.shape, lambda i: (0, 0, 0)),
        ],
        out_specs=(
            pl.BlockSpec((1, rows, 128), lambda i: (jnp.maximum(i - 1, 0), 0, 0)),
            pl.BlockSpec((4, 2, BLOCK), lambda i: (0, 0, jnp.maximum(i - 1, 0))),
        ),
        out_shape=(
            jax.ShapeDtypeStruct((blocks, rows, 128), BF16),
            jax.ShapeDtypeStruct((4, 2, length), F32),
        ),
        scratch_shapes=[
            pltpu.VMEM((3, rows, 128), F32),
            pltpu.VMEM((4, length, 128), BF16),
            pltpu.VMEM((4, length + 2 * BLOCK, 128), BF16),
            pltpu.VMEM((4, length + 2 * BLOCK, 256), BF16),
            pltpu.VMEM((length * 4, 128), F32),
            pltpu.VMEM((2 * BLOCK, 3 * BLOCK), F32),
            pltpu.VMEM((rows, 128), F32),
        ],
        compiler_params=pltpu.CompilerParams(dimension_semantics=("arbitrary",)),
        cost_estimate=pl.CostEstimate(flops=2 * 4096 * 2048 * 768, transcendentals=3 << 20, bytes_accessed=20 << 20),
        name="attn_branch",
    )(ids, scal, x, w, gain, before, after)


def out_kernel(yp_ref, ya_ref, wp_ref, wa_ref, o_ref):
    rows = yp_ref.shape[1]
    lanes_p = jnp.concatenate([yp_ref[j] for j in range(yp_ref.shape[0])], axis=1)
    lanes_a = jnp.concatenate([ya_ref[j] for j in range(ya_ref.shape[0])], axis=1)
    acc = jnp.dot(lanes_p, wp_ref[...], preferred_element_type=F32)
    acc = acc + jnp.dot(lanes_a, wa_ref[...], preferred_element_type=F32)
    o_ref.reshape(rows, o_ref.shape[2])[...] = acc.astype(BF16)


def out_matmul(y_pool, y_attn, w):
    parts, rows, cols = y_pool.shape
    width = w.shape[1] // 2
    tile = 512
    steps = width // tile
    return pl.pallas_call(
        out_kernel,
        grid=(steps,),
        in_specs=[
            pl.BlockSpec(y_pool.shape, lambda n: (0, 0, 0)),
            pl.BlockSpec(y_attn.shape, lambda n: (0, 0, 0)),
            pl.BlockSpec((parts * cols, tile), lambda n: (0, n)),
            pl.BlockSpec((parts * cols, tile), lambda n: (0, n + steps)),
        ],
        out_specs=pl.BlockSpec((rows // 4, 4, tile), lambda n: (0, 0, n)),
        out_shape=jax.ShapeDtypeStruct((rows // 4, 4, width), BF16),
        compiler_params=pltpu.CompilerParams(dimension_semantics=("arbitrary",)),
        cost_estimate=pl.CostEstimate(flops=2 * 512 * 2048 * 2048, transcendentals=0, bytes_accessed=12 << 20),
        name="out_matmul",
    )(y_pool, y_attn, w, w)


def body(
    inputs,
    norm_gain,
    pool_proj,
    pool_gate_proj,
    pool_mix,
    query_proj,
    key_proj,
    value_proj,
    attn_gate_proj,
    query_gain,
    key_gain,
    sink_logit,
    out_pool,
    out_attn,
):
    sp = lax.axis_index("sp")
    tp = lax.axis_index("tp")
    sp_size = lax.axis_size("sp")
    length = inputs.shape[0]
    out_w = lax.all_gather(jnp.concatenate([out_pool, out_attn], axis=1), "sp", axis=0, tiled=True)
    gain_col = norm_gain[:, None]

    def weighted(parts):
        return (jnp.concatenate(parts, axis=1).astype(F32) * gain_col).astype(BF16)

    w_edge = weighted([pool_proj, key_proj, value_proj])
    w_pool = weighted([pool_proj, pool_gate_proj])
    w_attn = weighted([query_proj, key_proj, key_proj, value_proj, value_proj, attn_gate_proj])
    gains = jnp.concatenate([query_gain * (LOG2E * HEAD_DIM**-0.5)] * 2 + [key_gain] * 2)[None, :]
    heads = tp * 2 + jnp.arange(2, dtype=jnp.int32)
    slopes = 2.0 ** (-8.0 * (heads + 1).astype(F32) / HEADS)
    shift = jnp.maximum(sink_logit, 0.0)
    scal = jnp.concatenate([slopes * LOG2E, shift * LOG2E, jnp.exp(sink_logit - shift), shift])
    ids = jnp.stack(
        [
            sp,
            tp % 4,
            jnp.int32(length * sp_size),
            (sp > 0).astype(jnp.int32),
            (sp < sp_size - 1).astype(jnp.int32),
        ]
    )
    edge = edges(inputs, w_edge)
    up = [(i, i + 1) for i in range(sp_size - 1)]
    down = [(j, i) for i, j in up]
    before = lax.ppermute(edge[1], "sp", up)
    after = lax.ppermute(edge[0], "sp", down)
    y_pool = pool_branch(ids, inputs, w_pool, pool_mix, before, after)
    pool_rows = lax.all_to_all(y_pool, "tp", split_axis=0, concat_axis=0, tiled=True)
    y_attn, lse = attn_branch(ids, scal, inputs, w_attn, gains, before, after)
    attn_rows = lax.all_to_all(y_attn, "tp", split_axis=0, concat_axis=0, tiled=True)
    mixed = out_matmul(pool_rows, attn_rows, out_w)
    return mixed, jnp.transpose(lse, (2, 0, 1))


def solution(mesh):
    placed = (
        P("sp", None, None),
        P(),
        P(None, "tp"),
        P(None, "tp"),
        P("tp", None, None),
        P(None, "tp"),
        P(None, "tp"),
        P(None, "tp"),
        P(None, "tp"),
        P(),
        P(),
        P("tp"),
        P("sp", None),
        P("sp", None),
    )
    return jax.shard_map(
        body,
        mesh=mesh,
        in_specs=placed,
        out_specs=(P(("sp", "tp"), None, None), P("sp", None, "tp")),
        check_vma=False,
    )
```

```python
import functools
import math

import jax
import jax.numpy as jnp
from jax import lax
from jax.experimental import pallas as pl
from jax.experimental.pallas import tpu as pltpu
from jax.sharding import PartitionSpec as P


HEAD_DIM = 64
WINDOW = 128
REACH = 8
EPS = 1e-06
NEG = -1e30
LOG2E = math.log2(math.e)
F32 = jnp.float32
BF16 = jnp.bfloat16
BLOCK = 128


def row_scale(x):
    width = x.shape[1]
    acc = None
    for c in range(0, width, 512):
        parts = [x[:, c + d : c + d + 128] for d in range(0, 512, 128)]
        parts = [p * p for p in parts]
        four = ((parts[0] + parts[1]) + (parts[2] + parts[3])).astype(F32)
        acc = four if acc is None else acc + four
    total = jnp.sum(acc, axis=-1, keepdims=True)
    return lax.rsqrt(total * (1.0 / width) + EPS)


def silu(v):
    return v / (1.0 + jnp.exp(-v))


def first_kernel(
    x_ref, gain_ref, pool_ref, pgate_ref, query_ref, keyt_ref, valuet_ref, agate_ref,
    head_ref, tail_ref, wp_ref, wa_ref, w_edge, scr, xs,
):
    half = x_ref.shape[0]
    step = pl.program_id(0)

    @pl.when(step == 0)
    def _():
        low = lax.broadcasted_iota(jnp.int32, (128, 128), 1) < HEAD_DIM
        for c in range(0, x_ref.shape[2], 128):
            rows = slice(c, c + 128)
            line = gain_ref[:, rows]
            column = jnp.broadcast_to(line, (128, 128)).T
            pool = (pool_ref[rows, :].astype(F32) * column).astype(BF16)
            wp_ref[rows, 0:128] = pool
            wp_ref[rows, 128:256] = (pgate_ref[rows, :].astype(F32) * column).astype(BF16)
            kv = (jnp.concatenate([keyt_ref[:, rows], valuet_ref[:, rows]], axis=0).astype(F32) * line).T
            turned = pltpu.roll(kv, HEAD_DIM, 1)
            wa_ref[rows, 0:128] = (query_ref[rows, :].astype(F32) * column).astype(BF16)
            wa_ref[rows, 128:256] = jnp.where(low, kv, turned).astype(BF16)
            wa_ref[rows, 256:384] = jnp.where(low, turned, kv).astype(BF16)
            wa_ref[rows, 384:512] = (agate_ref[rows, :].astype(F32) * column).astype(BF16)
            w_edge[rows, 0:128] = pool
            w_edge[rows, 128:256] = kv.astype(BF16)

    xs[...] = x_ref.reshape(half * 4, x_ref.shape[2])[...]
    x = xs[...]
    cols = jnp.dot(x, w_edge[...], preferred_element_type=F32) * row_scale(x)
    scr[0] = cols[:, :128]
    scr[1] = cols[:, 128:]
    for n in range(4):
        out = head_ref if n < 2 else tail_ref
        part = n % 2

        @pl.when(step == n)
        def _(n=n, out=out, part=part):
            for s in range(4):
                rows = scr[1, pl.ds(s, half, stride=4), :]
                out[s, part * half : (part + 1) * half, :] = rows.astype(BF16)
                if n == 0:
                    out[s, 128 : 128 + REACH, :] = scr[0, pl.ds(s, REACH, stride=4), :].astype(BF16)
                if n == 3:
                    rows = scr[0, pl.ds(s + 4 * (half - REACH), REACH, stride=4), :]
                    out[s, 128 : 128 + REACH, :] = rows.astype(BF16)


def first_rows(x, gain, pool, pgate, query, keyt, valuet, agate):
    half = 64
    width = x.shape[2]
    last = x.shape[0] // half
    whole = [gain, pool, pgate, query, keyt, valuet, agate]
    return pl.pallas_call(
        first_kernel,
        grid=(4,),
        in_specs=[pl.BlockSpec((half, 4, width), lambda i: (i + (last - 4) * (i // 2), 0, 0))]
        + [pl.BlockSpec(a.shape, lambda i: (0, 0)) for a in whole],
        out_specs=(
            pl.BlockSpec((4, 136, 128), lambda i: (0, 0, 0)),
            pl.BlockSpec((4, 136, 128), lambda i: (0, 0, 0)),
            pl.BlockSpec((width, 256), lambda i: (0, 0)),
            pl.BlockSpec((width, 512), lambda i: (0, 0)),
        ),
        out_shape=(
            jax.ShapeDtypeStruct((4, 136, 128), BF16),
            jax.ShapeDtypeStruct((4, 136, 128), BF16),
            jax.ShapeDtypeStruct((width, 256), BF16),
            jax.ShapeDtypeStruct((width, 512), BF16),
        ),
        scratch_shapes=[
            pltpu.VMEM((width, 256), BF16),
            pltpu.VMEM((2, half * 4, 128), F32),
            pltpu.VMEM((half * 4, width), BF16),
        ],
        compiler_params=pltpu.CompilerParams(dimension_semantics=("arbitrary",)),
        cost_estimate=pl.CostEstimate(flops=2 * 1024 * 2048 * 256, transcendentals=0, bytes_accessed=12 << 20),
        name="first_rows",
    )(x, *whole)


def pool_kernel(x_ref, w_ref, mix_ref, before_ref, after_ref, y_ref, pool, gate, inverse, xs, xv, sems):
    step = pl.program_id(0)
    blocks = pl.num_programs(0) - 1
    rows = BLOCK * 4
    pad = 64
    total_rows = blocks * rows
    length_blocks = xv.shape[0] // BLOCK
    power = lax.axis_index("tp") % 4
    half = jnp.left_shift(jnp.int32(1), power)

    def fetch(n):
        span = pl.ds(n * BLOCK, BLOCK)
        return pltpu.make_async_copy(x_ref.at[span], xv.at[span], sems.at[n])

    @pl.when(step == 0)
    def _():
        for n in range(length_blocks):
            fetch(n).start()
        for s in range(4):
            pool[pl.ds(pad - 4 * REACH + s, REACH, stride=4), :] = before_ref[s, 128 : 128 + REACH, :].astype(F32)
            pool[pl.ds(pad + total_rows + s, REACH, stride=4), :] = after_ref[s, 128 : 128 + REACH, :].astype(F32)
        length = blocks * BLOCK
        begin = lax.axis_index("sp") * length
        total = lax.axis_size("sp") * length
        for k in range(3):
            where = (0, BLOCK, length - BLOCK)[k]
            position = begin + where + lax.broadcasted_iota(jnp.int32, (rows, 128), 0) // 4
            count = jnp.minimum(position + half - 1, total - 1) - jnp.maximum(position - half, 0) + 1
            inverse[k] = 1.0 / count.astype(F32)

    def finish():
        at = pl.multiple_of((step - 1) * rows, rows)
        base = pad + at
        reach = 4 * REACH
        window = pool[pl.ds(base - reach, rows + 2 * reach), :]
        size = rows + 2 * reach - 8
        two = window[:size] + window[4 : size + 4]
        four = two[: size - 8] + two[8:]
        eight = four[: size - 24] + four[16 : size - 8]
        sixteen = eight[: size - 56] + eight[32 : size - 24]
        sums = jnp.where(
            power == 0,
            two[reach - 4 : reach - 4 + rows],
            jnp.where(
                power == 1,
                four[reach - 8 : reach - 8 + rows],
                jnp.where(power == 2, eight[reach - 16 : reach - 16 + rows], sixteen[:rows]),
            ),
        )
        kind = jnp.where(step == 1, 0, jnp.where(step == blocks, 2, 1))
        pooled = (sums * inverse[kind] - window[reach : reach + rows]).astype(BF16)
        mixed = jnp.dot(pooled, mix_ref[0], preferred_element_type=F32)
        y_ref[0] = (mixed * silu(gate[pl.ds(at, rows), :])).astype(BF16)

    def project():
        fetch(step).wait()
        xs[...] = xv.at[pl.ds(pl.multiple_of(step * BLOCK, BLOCK), BLOCK)].reshape(rows, xv.shape[2])[...]
        x = xs[...]
        both = jnp.dot(x, w_ref[...], preferred_element_type=F32) * row_scale(x)
        at = pl.multiple_of(step * rows, rows)
        pool[pl.ds(pad + at, rows), :] = both[:, :128]
        gate[pl.ds(at, rows), :] = both[:, 128:]

    @pl.when(step == 0)
    def _():
        project()

    @pl.when((step > 0) & (step < blocks))
    def _():
        project()
        finish()

    @pl.when(step == blocks)
    def _():
        finish()


def pool_branch(x, w, mix, before, after):
    length, _, width = x.shape
    blocks = length // BLOCK
    rows = BLOCK * 4
    return pl.pallas_call(
        pool_kernel,
        grid=(blocks + 1,),
        in_specs=[
            pl.BlockSpec(memory_space=pl.ANY),
            pl.BlockSpec(w.shape, lambda i: (0, 0)),
            pl.BlockSpec(mix.shape, lambda i: (0, 0, 0)),
            pl.BlockSpec(before.shape, lambda i: (0, 0, 0)),
            pl.BlockSpec(after.shape, lambda i: (0, 0, 0)),
        ],
        out_specs=pl.BlockSpec((1, rows, 128), lambda i: (jnp.maximum(i - 1, 0), 0, 0)),
        out_shape=jax.ShapeDtypeStruct((blocks, rows, 128), BF16),
        scratch_shapes=[
            pltpu.VMEM((length * 4 + 128, 128), F32),
            pltpu.VMEM((length * 4, 128), F32),
            pltpu.VMEM((3, rows, 128), F32),
            pltpu.VMEM((rows, width), BF16),
            pltpu.VMEM(x.shape, BF16),
            pltpu.SemaphoreType.DMA((blocks,)),
        ],
        compiler_params=pltpu.CompilerParams(dimension_semantics=("arbitrary",)),
        cost_estimate=pl.CostEstimate(flops=2 * 4096 * 2048 * 256, transcendentals=0, bytes_accessed=18 << 20),
        name="pool_branch",
    )(x, w, mix, before, after)


def attn_kernel(
    sink_ref, x_ref, w_ref, qgain_ref, kgain_ref, before_ref, after_ref, first_ref,
    y_ref, lse_ref, proj, qs, ks, vs, gate, bias, att, xs, sinks, gains,
):
    del first_ref
    step = pl.program_id(0)
    blocks = pl.num_programs(0) - 1
    rows = BLOCK * 4
    lane = lax.broadcasted_iota(jnp.int32, (BLOCK, 128), 1)
    low_lanes = lane < HEAD_DIM
    shifts = [jnp.maximum(sink_ref[h], 0.0) for h in range(2)]

    @pl.when(step == 0)
    def _():
        query = lax.broadcasted_iota(jnp.int32, (BLOCK, 3 * BLOCK), 0)
        key = lax.broadcasted_iota(jnp.int32, (BLOCK, 3 * BLOCK), 1) - BLOCK
        distance = jnp.abs(query - key)
        scale = lax.broadcasted_iota(jnp.int32, (BLOCK, 3 * BLOCK), 0) * 0 + jnp.left_shift(
            jnp.int32(1), lax.axis_index("tp")
        )
        for h in range(2):
            slope = ((0.5**0.5, 0.5)[h] * LOG2E) / scale.astype(F32)
            line = -slope * distance.astype(F32) - shifts[h] * LOG2E
            bias[h * BLOCK : (h + 1) * BLOCK, :] = jnp.where(distance <= WINDOW, line, NEG)
        shift_row = jnp.where(low_lanes, shifts[0], shifts[1])
        sink_row = jnp.where(low_lanes, sink_ref[0], sink_ref[1])
        sinks[...] = jnp.exp(sink_row - shift_row)
        qgain = qgain_ref[...] * (LOG2E * HEAD_DIM**-0.5)
        gains[...] = jnp.concatenate([qgain, qgain, kgain_ref[...], kgain_ref[...]], axis=1)
        key_gain = jnp.concatenate([kgain_ref[...], kgain_ref[...]], axis=1)
        sp = lax.axis_index("sp")
        for side, ref in enumerate((before_ref, after_ref)):
            at = 0 if side == 0 else (blocks + 1) * BLOCK
            live = (sp > 0) if side == 0 else (sp < lax.axis_size("sp") - 1)
            live = jnp.where(live, 1.0, 0.0)
            for s in range(4):
                kv = ref[s, 0:128, :].astype(F32)
                turned = pltpu.roll(kv, HEAD_DIM, 1)
                kk = jnp.where(low_lanes, kv, turned)
                vv = jnp.where(low_lanes, turned, kv)
                mean = jnp.sum(jnp.where(low_lanes, kv * kv, 0.0), axis=-1, keepdims=True) * (1.0 / HEAD_DIM)
                ks[s, pl.ds(at, BLOCK), :] = (kk * lax.rsqrt(mean + EPS) * key_gain).astype(BF16)
                vs[s, pl.ds(at, BLOCK), 0:128] = vv.astype(BF16)
                vs[s, pl.ds(at, BLOCK), 128:256] = jnp.full((BLOCK, 128), live, F32).astype(BF16)

    def project(part):
        size = rows // 2
        at = part * size
        xs[at : at + size, :] = x_ref.at[part * (BLOCK // 2) : (part + 1) * (BLOCK // 2)].reshape(size, x_ref.shape[2])[...]
        x = xs[at : at + size, :]
        cols = jnp.dot(x, w_ref[...], preferred_element_type=F32) * row_scale(x)
        qk = cols[:, :256]
        r = lax.broadcasted_iota(jnp.int32, (256, 256), 0) // HEAD_DIM
        c = lax.broadcasted_iota(jnp.int32, (256, 256), 1) // HEAD_DIM
        same = jnp.where(r == c, 1.0, 0.0).astype(BF16)
        squares = jnp.dot((qk * qk).astype(BF16), same, preferred_element_type=F32)
        normed = qk * lax.rsqrt(squares * (1.0 / HEAD_DIM) + EPS) * gains[...]
        proj[0, at : at + size] = normed[:, :128]
        proj[1, at : at + size] = normed[:, 128:]
        proj[2, at : at + size] = cols[:, 256:384]
        gate[step % 2, at : at + size, :] = cols[:, 384:]

    def separate():
        at = pl.multiple_of(step * BLOCK, BLOCK)
        for s in range(4):
            mine = pl.ds(s, BLOCK, stride=4)
            qs[step % 2, s] = proj[0, mine, :].astype(BF16)
            ks[s, pl.ds(at + BLOCK, BLOCK), :] = proj[1, mine, :].astype(BF16)
            vs[s, pl.ds(at + BLOCK, BLOCK), 0:128] = proj[2, mine, :].astype(BF16)
            vs[s, pl.ds(at + BLOCK, BLOCK), 128:256] = jnp.ones((BLOCK, 128), BF16)

    def attend(s):
        at = pl.multiple_of((step - 1) * BLOCK, BLOCK)
        q = qs[(step - 1) % 2, s]
        zero = jnp.zeros_like(q)
        two = jnp.concatenate([jnp.where(low_lanes, q, zero), jnp.where(low_lanes, zero, q)], axis=0)
        keys = ks[s, pl.ds(at, 3 * BLOCK), :]
        score = lax.dot_general(two, keys, (((1,), (1,)), ((), ())), preferred_element_type=F32)
        weight = jnp.exp2(score + bias[...]).astype(BF16)
        out = jnp.dot(weight, vs[s, pl.ds(at, 3 * BLOCK), :], preferred_element_type=F32)
        total = jnp.where(low_lanes, out[:BLOCK, 128:], out[BLOCK:, 128:]) + sinks[...]
        value = jnp.where(low_lanes, out[:BLOCK, :128], out[BLOCK:, :128])
        att[pl.ds(s, BLOCK, stride=4), :] = value / total
        turned = total.T
        lse_ref[s, 0:1, :] = jnp.log(turned[0:1, :]) + shifts[0]
        lse_ref[s, 1:2, :] = jnp.log(turned[HEAD_DIM : HEAD_DIM + 1, :]) + shifts[1]

    def close():
        y_ref[0] = (att[...] * silu(gate[(step - 1) % 2])).astype(BF16)

    @pl.when(step < blocks)
    def _():
        project(0)
        project(1)
        separate()

    @pl.when(step > 0)
    def _():
        for s in range(4):
            attend(s)
        close()


def attn_branch(sink, x, w, qgain, kgain, before, after, first):
    length, _, width = x.shape
    blocks = length // BLOCK
    rows = BLOCK * 4
    return pl.pallas_call(
        attn_kernel,
        grid=(blocks + 1,),
        in_specs=[
            pl.BlockSpec(memory_space=pltpu.SMEM),
            pl.BlockSpec((BLOCK, 4, width), lambda i: (jnp.minimum(i, blocks - 1), 0, 0)),
            pl.BlockSpec(w.shape, lambda i: (0, 0)),
            pl.BlockSpec(qgain.shape, lambda i: (0, 0)),
            pl.BlockSpec(kgain.shape, lambda i: (0, 0)),
            pl.BlockSpec(before.shape, lambda i: (0, 0, 0)),
            pl.BlockSpec(after.shape, lambda i: (0, 0, 0)),
            pl.BlockSpec(memory_space=pl.ANY),
        ],
        out_specs=(
            pl.BlockSpec((1, rows, 128), lambda i: (jnp.maximum(i - 1, 0), 0, 0)),
            pl.BlockSpec((4, 2, BLOCK), lambda i: (0, 0, jnp.maximum(i - 1, 0))),
        ),
        out_shape=(
            jax.ShapeDtypeStruct((blocks, rows, 128), BF16),
            jax.ShapeDtypeStruct((4, 2, length), F32),
        ),
        scratch_shapes=[
            pltpu.VMEM((3, rows, 128), F32),
            pltpu.VMEM((2, 4, BLOCK, 128), BF16),
            pltpu.VMEM((4, length + 2 * BLOCK, 128), BF16),
            pltpu.VMEM((4, length + 2 * BLOCK, 256), BF16),
            pltpu.VMEM((2, rows, 128), F32),
            pltpu.VMEM((2 * BLOCK, 3 * BLOCK), F32),
            pltpu.VMEM((rows, 128), F32),
            pltpu.VMEM((rows, width), BF16),
            pltpu.VMEM((BLOCK, 128), F32),
            pltpu.VMEM((1, 256), F32),
        ],
        compiler_params=pltpu.CompilerParams(dimension_semantics=("arbitrary",)),
        cost_estimate=pl.CostEstimate(flops=2 * 4096 * 2048 * 768, transcendentals=3 << 20, bytes_accessed=20 << 20),
        name="attn_branch",
    )(sink, x, w, qgain, kgain, before, after, first)


def half_kernel(which, y_ref, *rest):
    pieces, rest = rest[:8], rest[8:]
    add_ref, (o_ref, w, sems) = (None, rest) if which == 0 else (rest[0], rest[1:])
    tiles, _, tile = w.shape
    rows = y_ref.shape[1]
    step = pl.program_id(0)
    place = lax.axis_index("sp")
    z, y, core = place // 4, place % 4, lax.axis_index("tp") % 2

    def copies(n, side):
        for m in range(4):
            for k in range(4):
                a = (z + 4 - (m if which == 0 else k)) % 4
                b = (y + 4 - (k if which == 0 else m)) % 4
                row = pl.multiple_of((a * 4 + b) * 64, 64)
                yield pltpu.make_async_copy(
                    pieces[side * 4 + m].at[pl.ds(k * 64, 64), pl.ds(n * tile, tile)],
                    w.at[n, pl.ds(row, 64), :],
                    sems.at[n, m * 4 + k],
                )

    for side in range(2):

        @pl.when((step == 0) & (core == (which if side == 0 else 1 - which)))
        def _(side=side):
            for n in range(tiles):
                for copy in copies(n, side):
                    copy.start()

    for n in range(tiles):

        @pl.when(step == n)
        def _(n=n):
            for copy in copies(n, 0):
                copy.wait()

    lanes = jnp.concatenate([y_ref[j] for j in range(y_ref.shape[0])], axis=1)
    acc = jnp.dot(lanes, w[step], preferred_element_type=F32)
    if which == 0:
        o_ref[...] = acc
    else:
        o_ref.reshape(rows, tile)[...] = (acc + add_ref[...]).astype(BF16)


def half_matmul(which, y, pieces, add=None):
    parts, rows, cols = y.shape
    width = pieces[0].shape[1]
    tile = 512
    steps = width // tile
    if which == 0:
        out_spec = pl.BlockSpec((rows, tile), lambda n: (0, n))
        out_shape = jax.ShapeDtypeStruct((rows, width), F32)
    else:
        out_spec = pl.BlockSpec((rows // 4, 4, tile), lambda n: (0, 0, n))
        out_shape = jax.ShapeDtypeStruct((rows // 4, 4, width), BF16)
    return pl.pallas_call(
        functools.partial(half_kernel, which),
        grid=(steps,),
        in_specs=[pl.BlockSpec(y.shape, lambda n: (0, 0, 0))]
        + [pl.BlockSpec(memory_space=pl.ANY)] * 8
        + ([pl.BlockSpec((rows, tile), lambda n: (0, n))] if which else []),
        out_specs=out_spec,
        out_shape=out_shape,
        scratch_shapes=[
            pltpu.VMEM((steps, parts * cols, tile), BF16),
            pltpu.SemaphoreType.DMA((steps, 16)),
        ],
        compiler_params=pltpu.CompilerParams(dimension_semantics=("arbitrary",)),
        cost_estimate=pl.CostEstimate(flops=512 * 2048 * 2048, transcendentals=0, bytes_accessed=8 << 20),
    )(y, *pieces, *([add] if which else []))


def ring_pairs(shift, first):
    pairs = []
    for z in range(4):
        for y in range(4):
            for t in range(8):
                along_y = (t % 2 == 0) == first
                to = (z, (y + shift) % 4) if along_y else ((z + shift) % 4, y)
                pairs.append(((z * 4 + y) * 8 + t, (to[0] * 4 + to[1]) * 8 + t))
    return pairs


def gather_weights(out_pool, out_attn, core):
    both = ("sp", "tp")
    half = jnp.where(core == 0, out_pool, out_attn)
    return [half] + [lax.ppermute(half, both, ring_pairs(k, True)) for k in (1, 2, 3)]


def gather_rest(line):
    both = ("sp", "tp")
    block = jnp.concatenate(line, axis=0)
    mine = [block] + [lax.ppermute(block, both, ring_pairs(k, False)) for k in (1, 2, 3)]
    swap = [(i, i ^ 1) for i in range(8)]
    return mine + [lax.ppermute(piece, "tp", swap) for piece in mine]


def body(
    inputs,
    norm_gain,
    pool_proj,
    pool_gate_proj,
    pool_mix,
    query_proj,
    key_proj,
    value_proj,
    attn_gate_proj,
    query_gain,
    key_gain,
    sink_logit,
    out_pool,
    out_attn,
):
    tp = lax.axis_index("tp")
    sp_size = lax.axis_size("sp")
    core = tp % 2
    line = gather_weights(out_pool, out_attn, core)
    head, tail, w_pool, w_attn = first_rows(
        inputs, norm_gain[None, :], pool_proj, pool_gate_proj, query_proj, key_proj.T, value_proj.T, attn_gate_proj
    )
    up = [(i, i + 1) for i in range(sp_size - 1)]
    down = [(j, i) for i, j in up]
    *line, head, tail = lax.optimization_barrier((*line, head, tail))
    before = lax.ppermute(tail, "sp", up)
    after = lax.ppermute(head, "sp", down)
    pieces = gather_rest(line)
    y_pool = pool_branch(inputs, w_pool, pool_mix, before, after)
    pool_rows = lax.all_to_all(y_pool, "tp", split_axis=0, concat_axis=0, tiled=True)
    y_attn, lse = attn_branch(
        sink_logit, inputs, w_attn, query_gain[None, :], key_gain[None, :], before, after, y_pool
    )
    y_attn, pool_rows = lax.optimization_barrier((y_attn, pool_rows))
    attn_rows = lax.all_to_all(y_attn, "tp", split_axis=0, concat_axis=0, tiled=True)
    partial = half_matmul(0, pool_rows, pieces)
    mixed = half_matmul(1, attn_rows, pieces, partial)
    return mixed, jnp.transpose(lse, (2, 0, 1))


def solution(mesh):
    placed = (
        P("sp", None, None),
        P(),
        P(None, "tp"),
        P(None, "tp"),
        P("tp", None, None),
        P(None, "tp"),
        P(None, "tp"),
        P(None, "tp"),
        P(None, "tp"),
        P(),
        P(),
        P("tp"),
        P("sp", None),
        P("sp", None),
    )

    return jax.shard_map(
        body,
        mesh=mesh,
        in_specs=placed,
        out_specs=(P(("sp", "tp"), None, None), P("sp", None, "tp")),
        check_vma=False,
    )
```

```python
import functools
import math

import jax
import jax.numpy as jnp
from jax import lax
from jax.experimental import pallas as pl
from jax.experimental.pallas import tpu as pltpu
from jax.sharding import PartitionSpec as P

HEAD_DIM = 64
WINDOW = 128
REACH = 8
EPS = 1e-06
NEG = -1e30
LOG2E = math.log2(math.e)
F32 = jnp.float32
BF16 = jnp.bfloat16
BLOCK = 128


def row_scale(x):
    width = x.shape[1]
    acc = None
    for c in range(0, width, 512):
        parts = [x[:, c + d : c + d + 128] for d in range(0, 512, 128)]
        parts = [p * p for p in parts]
        four = ((parts[0] + parts[1]) + (parts[2] + parts[3])).astype(F32)
        acc = four if acc is None else acc + four
    total = jnp.sum(acc, axis=-1, keepdims=True)
    return lax.rsqrt(total * (1.0 / width) + EPS)


def silu(v):
    return v / (1.0 + jnp.exp(-v))


def first_kernel(
    x_ref, gain_ref, pool_ref, pgate_ref, query_ref, keyt_ref, valuet_ref, agate_ref,
    head_ref, tail_ref, wp_out, wa_out, w_edge, scr, xs, wp_ref, wa_ref, sems,
):
    half = x_ref.shape[0]
    step = pl.program_id(0)
    leave = [pltpu.make_async_copy(a, b, sems.at[n]) for n, (a, b) in enumerate(((wp_ref, wp_out), (wa_ref, wa_out)))]

    @pl.when(step == 0)
    def _():
        low = lax.broadcasted_iota(jnp.int32, (128, 128), 1) < HEAD_DIM
        for c in range(0, x_ref.shape[2], 128):
            rows = slice(c, c + 128)
            line = gain_ref[:, rows]
            column = jnp.broadcast_to(line, (128, 128)).T
            pool = (pool_ref[rows, :].astype(F32) * column).astype(BF16)
            wp_ref[rows, 0:128] = pool
            wp_ref[rows, 128:256] = (pgate_ref[rows, :].astype(F32) * column).astype(BF16)
            kv = (jnp.concatenate([keyt_ref[:, rows], valuet_ref[:, rows]], axis=0).astype(F32) * line).T
            turned = pltpu.roll(kv, HEAD_DIM, 1)
            wa_ref[rows, 0:128] = (query_ref[rows, :].astype(F32) * column).astype(BF16)
            wa_ref[rows, 128:256] = jnp.where(low, kv, turned).astype(BF16)
            wa_ref[rows, 256:384] = jnp.where(low, turned, kv).astype(BF16)
            wa_ref[rows, 384:512] = (agate_ref[rows, :].astype(F32) * column).astype(BF16)
            w_edge[rows, 0:128] = pool
            w_edge[rows, 128:256] = kv.astype(BF16)
        for copy in leave:
            copy.start()

    xs[...] = x_ref.reshape(half * 4, x_ref.shape[2])[...]
    x = xs[...]
    cols = jnp.dot(x, w_edge[...], preferred_element_type=F32) * row_scale(x)
    scr[0] = cols[:, :128]
    scr[1] = cols[:, 128:]
    for n in range(4):
        out = head_ref if n < 2 else tail_ref
        part = n % 2

        @pl.when(step == n)
        def _(n=n, out=out, part=part):
            for s in range(4):
                rows = scr[1, pl.ds(s, half, stride=4), :]
                out[s, part * half : (part + 1) * half, :] = rows.astype(BF16)
                if n == 0:
                    out[s, 128 : 128 + REACH, :] = scr[0, pl.ds(s, REACH, stride=4), :].astype(BF16)
                if n == 3 and s == 0:
                    for copy in leave:
                        copy.wait()
                if n == 3:
                    rows = scr[0, pl.ds(s + 4 * (half - REACH), REACH, stride=4), :]
                    out[s, 128 : 128 + REACH, :] = rows.astype(BF16)


def first_rows(x, gain, pool, pgate, query, keyt, valuet, agate):
    half = 64
    width = x.shape[2]
    last = x.shape[0] // half
    whole = [gain, pool, pgate, query, keyt, valuet, agate]
    return pl.pallas_call(
        first_kernel,
        grid=(4,),
        in_specs=[pl.BlockSpec((half, 4, width), lambda i: (i + (last - 4) * (i // 2), 0, 0))]
        + [pl.BlockSpec(a.shape, lambda i: (0, 0)) for a in whole],
        out_specs=(
            pl.BlockSpec((4, 136, 128), lambda i: (0, 0, 0)),
            pl.BlockSpec((4, 136, 128), lambda i: (0, 0, 0)),
            pl.BlockSpec(memory_space=pl.ANY),
            pl.BlockSpec(memory_space=pl.ANY),
        ),
        out_shape=(
            jax.ShapeDtypeStruct((4, 136, 128), BF16),
            jax.ShapeDtypeStruct((4, 136, 128), BF16),
            jax.ShapeDtypeStruct((width, 256), BF16),
            jax.ShapeDtypeStruct((width, 512), BF16),
        ),
        scratch_shapes=[
            pltpu.VMEM((width, 256), BF16),
            pltpu.VMEM((2, half * 4, 128), F32),
            pltpu.VMEM((half * 4, width), BF16),
            pltpu.VMEM((width, 256), BF16),
            pltpu.VMEM((width, 512), BF16),
            pltpu.SemaphoreType.DMA((2,)),
        ],
        compiler_params=pltpu.CompilerParams(dimension_semantics=("arbitrary",)),
        cost_estimate=pl.CostEstimate(flops=2 * 1024 * 2048 * 256, transcendentals=0, bytes_accessed=12 << 20),
        name="first_rows",
    )(x, *whole)


def pool_kernel(x_ref, w_ref, mix_ref, before_ref, after_ref, y_ref, scale_ref, pool, gate, inverse, xs, xv, sems):
    step = pl.program_id(0)
    blocks = pl.num_programs(0) - 1
    rows = BLOCK * 4
    pad = 64
    total_rows = blocks * rows
    length_blocks = xv.shape[0] // BLOCK
    power = lax.axis_index("tp") % 4
    half = jnp.left_shift(jnp.int32(1), power)

    def fetch(n):
        span = pl.ds(n * BLOCK, BLOCK)
        return pltpu.make_async_copy(x_ref.at[span], xv.at[span], sems.at[n])

    @pl.when(step == 0)
    def _():
        for n in range(length_blocks):
            fetch(n).start()
        for s in range(4):
            pool[pl.ds(pad - 4 * REACH + s, REACH, stride=4), :] = before_ref[s, 128 : 128 + REACH, :].astype(F32)
            pool[pl.ds(pad + total_rows + s, REACH, stride=4), :] = after_ref[s, 128 : 128 + REACH, :].astype(F32)
        length = blocks * BLOCK
        begin = lax.axis_index("sp") * length
        total = lax.axis_size("sp") * length
        for k in range(3):
            where = (0, BLOCK, length - BLOCK)[k]
            position = begin + where + lax.broadcasted_iota(jnp.int32, (rows, 128), 0) // 4
            count = jnp.minimum(position + half - 1, total - 1) - jnp.maximum(position - half, 0) + 1
            inverse[k] = 1.0 / count.astype(F32)

    def finish():
        at = pl.multiple_of((step - 1) * rows, rows)
        base = pad + at
        reach = 4 * REACH
        window = pool[pl.ds(base - reach, rows + 2 * reach), :]
        size = rows + 2 * reach - 8
        two = window[:size] + window[4 : size + 4]
        four = two[: size - 8] + two[8:]
        eight = four[: size - 24] + four[16 : size - 8]
        sixteen = eight[: size - 56] + eight[32 : size - 24]
        sums = jnp.where(
            power == 0,
            two[reach - 4 : reach - 4 + rows],
            jnp.where(
                power == 1,
                four[reach - 8 : reach - 8 + rows],
                jnp.where(power == 2, eight[reach - 16 : reach - 16 + rows], sixteen[:rows]),
            ),
        )
        kind = jnp.where(step == 1, 0, jnp.where(step == blocks, 2, 1))
        pooled = (sums * inverse[kind] - window[reach : reach + rows]).astype(BF16)
        mixed = jnp.dot(pooled, mix_ref[0], preferred_element_type=F32)
        y_ref[0] = (mixed * silu(gate[pl.ds(at, rows), :])).astype(BF16)

    def project():
        fetch(step).wait()
        xs[...] = xv.at[pl.ds(pl.multiple_of(step * BLOCK, BLOCK), BLOCK)].reshape(rows, xv.shape[2])[...]
        x = xs[...]
        scale = row_scale(x)
        scale_ref[...] = jnp.broadcast_to(scale, (rows, 128))
        both = jnp.dot(x, w_ref[...], preferred_element_type=F32) * scale
        at = pl.multiple_of(step * rows, rows)
        pool[pl.ds(pad + at, rows), :] = both[:, :128]
        gate[pl.ds(at, rows), :] = both[:, 128:]

    @pl.when(step == 0)
    def _():
        project()

    @pl.when((step > 0) & (step < blocks))
    def _():
        project()
        finish()

    @pl.when(step == blocks)
    def _():
        finish()


def pool_branch(x, w, mix, before, after):
    length, _, width = x.shape
    blocks = length // BLOCK
    rows = BLOCK * 4
    return pl.pallas_call(
        pool_kernel,
        grid=(blocks + 1,),
        in_specs=[
            pl.BlockSpec(memory_space=pl.ANY),
            pl.BlockSpec(w.shape, lambda i: (0, 0)),
            pl.BlockSpec(mix.shape, lambda i: (0, 0, 0)),
            pl.BlockSpec(before.shape, lambda i: (0, 0, 0)),
            pl.BlockSpec(after.shape, lambda i: (0, 0, 0)),
        ],
        out_specs=(
            pl.BlockSpec((1, rows, 128), lambda i: (jnp.maximum(i - 1, 0), 0, 0)),
            pl.BlockSpec((rows, 128), lambda i: (jnp.minimum(i, blocks - 1), 0)),
        ),
        out_shape=(
            jax.ShapeDtypeStruct((blocks, rows, 128), BF16),
            jax.ShapeDtypeStruct((length * 4, 128), F32),
        ),
        scratch_shapes=[
            pltpu.VMEM((length * 4 + 128, 128), F32),
            pltpu.VMEM((length * 4, 128), F32),
            pltpu.VMEM((3, rows, 128), F32),
            pltpu.VMEM((rows, width), BF16),
            pltpu.VMEM(x.shape, BF16),
            pltpu.SemaphoreType.DMA((blocks,)),
        ],
        compiler_params=pltpu.CompilerParams(dimension_semantics=("arbitrary",)),
        cost_estimate=pl.CostEstimate(flops=2 * 4096 * 2048 * 256, transcendentals=0, bytes_accessed=18 << 20),
        name="pool_branch",
    )(x, w, mix, before, after)


def attn_kernel(
    sink_ref, x_ref, scale_ref, w_ref, qgain_ref, kgain_ref, before_ref, after_ref,
    y_ref, lse_ref, proj, qs, ks, vs, gate, bias, att, xs, sinks, gains, same,
):
    step = pl.program_id(0)
    blocks = pl.num_programs(0) - 1
    rows = BLOCK * 4
    lane = lax.broadcasted_iota(jnp.int32, (BLOCK, 128), 1)
    low_lanes = lane < HEAD_DIM
    shifts = [jnp.maximum(sink_ref[h], 0.0) for h in range(2)]

    @pl.when(step == 0)
    def _():
        query = lax.broadcasted_iota(jnp.int32, (BLOCK, 3 * BLOCK), 0)
        key = lax.broadcasted_iota(jnp.int32, (BLOCK, 3 * BLOCK), 1) - BLOCK
        distance = jnp.abs(query - key)
        r = lax.broadcasted_iota(jnp.int32, (256, 256), 0) // HEAD_DIM
        c = lax.broadcasted_iota(jnp.int32, (256, 256), 1) // HEAD_DIM
        same[...] = jnp.where(r == c, 1.0, 0.0).astype(BF16)
        scale = lax.broadcasted_iota(jnp.int32, (BLOCK, 3 * BLOCK), 0) * 0 + jnp.left_shift(
            jnp.int32(1), lax.axis_index("tp")
        )
        for h in range(2):
            slope = ((0.5**0.5, 0.5)[h] * LOG2E) / scale.astype(F32)
            line = -slope * distance.astype(F32) - shifts[h] * LOG2E
            bias[h * BLOCK : (h + 1) * BLOCK, :] = jnp.where(distance <= WINDOW, line, NEG)
        shift_row = jnp.where(low_lanes, shifts[0], shifts[1])
        sink_row = jnp.where(low_lanes, sink_ref[0], sink_ref[1])
        sinks[...] = jnp.exp(sink_row - shift_row)
        qgain = qgain_ref[...] * (LOG2E * HEAD_DIM**-0.5)
        gains[...] = jnp.concatenate([qgain, qgain, kgain_ref[...], kgain_ref[...]], axis=1)
        key_gain = jnp.concatenate([kgain_ref[...], kgain_ref[...]], axis=1)
        sp = lax.axis_index("sp")
        for side, ref in enumerate((before_ref, after_ref)):
            at = 0 if side == 0 else (blocks + 1) * BLOCK
            live = (sp > 0) if side == 0 else (sp < lax.axis_size("sp") - 1)
            live = jnp.where(live, 1.0, 0.0)
            for s in range(4):
                kv = ref[s, 0:128, :].astype(F32)
                turned = pltpu.roll(kv, HEAD_DIM, 1)
                kk = jnp.where(low_lanes, kv, turned)
                vv = jnp.where(low_lanes, turned, kv)
                mean = jnp.sum(jnp.where(low_lanes, kv * kv, 0.0), axis=-1, keepdims=True) * (1.0 / HEAD_DIM)
                ks[s, pl.ds(at, BLOCK), :] = (kk * lax.rsqrt(mean + EPS) * key_gain).astype(BF16)
                vs[s, pl.ds(at, BLOCK), 0:128] = vv.astype(BF16)
                vs[s, pl.ds(at, BLOCK), 128:256] = jnp.full((BLOCK, 128), live, F32).astype(BF16)

    def project(part):
        size = rows // 2
        at = part * size
        xs[at : at + size, :] = x_ref.at[part * (BLOCK // 2) : (part + 1) * (BLOCK // 2)].reshape(size, x_ref.shape[2])[...]
        x = xs[at : at + size, :]
        cols = jnp.dot(x, w_ref[...], preferred_element_type=F32)
        scale = scale_ref[at : at + size, :]
        qk = cols[:, :256] * jnp.concatenate([scale, scale], axis=1)
        squares = jnp.dot((qk * qk).astype(BF16), same[...], preferred_element_type=F32)
        normed = qk * lax.rsqrt(squares * (1.0 / HEAD_DIM) + EPS) * gains[...]
        proj[0, at : at + size] = normed[:, :128]
        proj[1, at : at + size] = normed[:, 128:]
        proj[2, at : at + size] = cols[:, 256:384] * scale
        gate[step % 2, at : at + size, :] = cols[:, 384:] * scale

    def separate():
        at = pl.multiple_of(step * BLOCK, BLOCK)
        for s in range(4):
            mine = pl.ds(s, BLOCK, stride=4)
            qs[step % 2, s] = proj[0, mine, :].astype(BF16)
            ks[s, pl.ds(at + BLOCK, BLOCK), :] = proj[1, mine, :].astype(BF16)
            vs[s, pl.ds(at + BLOCK, BLOCK), 0:128] = proj[2, mine, :].astype(BF16)
            vs[s, pl.ds(at + BLOCK, BLOCK), 128:256] = jnp.ones((BLOCK, 128), BF16)

    def attend(s):
        at = pl.multiple_of((step - 1) * BLOCK, BLOCK)
        q = qs[(step - 1) % 2, s]
        zero = jnp.zeros_like(q)
        two = jnp.concatenate([jnp.where(low_lanes, q, zero), jnp.where(low_lanes, zero, q)], axis=0)
        keys = ks[s, pl.ds(at, 3 * BLOCK), :]
        score = lax.dot_general(two, keys, (((1,), (1,)), ((), ())), preferred_element_type=F32)
        weight = jnp.exp2(score + bias[...]).astype(BF16)
        out = jnp.dot(weight, vs[s, pl.ds(at, 3 * BLOCK), :], preferred_element_type=F32)
        total = jnp.where(low_lanes, out[:BLOCK, 128:], out[BLOCK:, 128:]) + sinks[...]
        value = jnp.where(low_lanes, out[:BLOCK, :128], out[BLOCK:, :128])
        att[pl.ds(s, BLOCK, stride=4), :] = value / total
        turned = total.T
        lse_ref[s, 0:1, :] = jnp.log(turned[0:1, :]) + shifts[0]
        lse_ref[s, 1:2, :] = jnp.log(turned[HEAD_DIM : HEAD_DIM + 1, :]) + shifts[1]

    def close():
        y_ref[0] = (att[...] * silu(gate[(step - 1) % 2])).astype(BF16)

    @pl.when(step < blocks)
    def _():
        project(0)
        project(1)
        separate()

    @pl.when(step > 0)
    def _():
        for s in range(4):
            attend(s)
        close()


def attn_branch(sink, x, scale, w, qgain, kgain, before, after):
    length, _, width = x.shape
    blocks = length // BLOCK
    rows = BLOCK * 4
    return pl.pallas_call(
        attn_kernel,
        grid=(blocks + 1,),
        in_specs=[
            pl.BlockSpec(memory_space=pltpu.SMEM),
            pl.BlockSpec((BLOCK, 4, width), lambda i: (jnp.minimum(i, blocks - 1), 0, 0)),
            pl.BlockSpec((rows, 128), lambda i: (jnp.minimum(i, blocks - 1), 0)),
            pl.BlockSpec(w.shape, lambda i: (0, 0)),
            pl.BlockSpec(qgain.shape, lambda i: (0, 0)),
            pl.BlockSpec(kgain.shape, lambda i: (0, 0)),
            pl.BlockSpec(before.shape, lambda i: (0, 0, 0)),
            pl.BlockSpec(after.shape, lambda i: (0, 0, 0)),
        ],
        out_specs=(
            pl.BlockSpec((1, rows, 128), lambda i: (jnp.maximum(i - 1, 0), 0, 0)),
            pl.BlockSpec((4, 2, BLOCK), lambda i: (0, 0, jnp.maximum(i - 1, 0))),
        ),
        out_shape=(
            jax.ShapeDtypeStruct((blocks, rows, 128), BF16),
            jax.ShapeDtypeStruct((4, 2, length), F32),
        ),
        scratch_shapes=[
            pltpu.VMEM((3, rows, 128), F32),
            pltpu.VMEM((2, 4, BLOCK, 128), BF16),
            pltpu.VMEM((4, length + 2 * BLOCK, 128), BF16),
            pltpu.VMEM((4, length + 2 * BLOCK, 256), BF16),
            pltpu.VMEM((2, rows, 128), F32),
            pltpu.VMEM((2 * BLOCK, 3 * BLOCK), F32),
            pltpu.VMEM((rows, 128), F32),
            pltpu.VMEM((rows, width), BF16),
            pltpu.VMEM((BLOCK, 128), F32),
            pltpu.VMEM((1, 256), F32),
            pltpu.VMEM((256, 256), BF16),
        ],
        compiler_params=pltpu.CompilerParams(dimension_semantics=("arbitrary",)),
        cost_estimate=pl.CostEstimate(flops=2 * 4096 * 2048 * 768, transcendentals=3 << 20, bytes_accessed=20 << 20),
        name="attn_branch",
    )(sink, x, scale, w, qgain, kgain, before, after)


def half_kernel(which, y_ref, *rest):
    pieces, rest = rest[:8], rest[8:]
    add_ref, (o_ref, w, sems) = (None, rest) if which == 0 else (rest[0], rest[1:])
    tiles, _, tile = w.shape
    rows = y_ref.shape[1]
    step = pl.program_id(0)
    place = lax.axis_index("sp")
    z, y, core = place // 4, place % 4, lax.axis_index("tp") % 2

    def copies(n, side):
        for m in range(4):
            for k in range(4):
                a = (z + 4 - (m if which == 0 else k)) % 4
                b = (y + 4 - (k if which == 0 else m)) % 4
                row = pl.multiple_of((a * 4 + b) * 64, 64)
                yield pltpu.make_async_copy(
                    pieces[side * 4 + m].at[pl.ds(k * 64, 64), pl.ds(n * tile, tile)],
                    w.at[n, pl.ds(row, 64), :],
                    sems.at[n, m * 4 + k],
                )

    for side in range(2):

        @pl.when((step == 0) & (core == (which if side == 0 else 1 - which)))
        def _(side=side):
            for n in range(tiles):
                for copy in copies(n, side):
                    copy.start()

    for n in range(tiles):

        @pl.when(step == n)
        def _(n=n):
            for copy in copies(n, 0):
                copy.wait()

    lanes = jnp.concatenate([y_ref[j] for j in range(y_ref.shape[0])], axis=1)
    acc = jnp.dot(lanes, w[step], preferred_element_type=F32)
    if which == 0:
        o_ref[...] = acc
    else:
        o_ref.reshape(rows, tile)[...] = (acc + add_ref[...]).astype(BF16)


def half_matmul(which, y, pieces, add=None):
    parts, rows, cols = y.shape
    width = pieces[0].shape[1]
    tile = 512
    steps = width // tile
    if which == 0:
        out_spec = pl.BlockSpec((rows, tile), lambda n: (0, n))
        out_shape = jax.ShapeDtypeStruct((rows, width), F32)
    else:
        out_spec = pl.BlockSpec((rows // 4, 4, tile), lambda n: (0, 0, n))
        out_shape = jax.ShapeDtypeStruct((rows // 4, 4, width), BF16)
    return pl.pallas_call(
        functools.partial(half_kernel, which),
        grid=(steps,),
        in_specs=[pl.BlockSpec(memory_space=pltpu.VMEM)]
        + [pl.BlockSpec(memory_space=pl.ANY)] * 8
        + ([pl.BlockSpec((rows, tile), lambda n: (0, n))] if which else []),
        out_specs=out_spec,
        out_shape=out_shape,
        scratch_shapes=[
            pltpu.VMEM((steps, parts * cols, tile), BF16),
            pltpu.SemaphoreType.DMA((steps, 16)),
        ],
        compiler_params=pltpu.CompilerParams(dimension_semantics=("arbitrary",)),
        cost_estimate=pl.CostEstimate(flops=512 * 2048 * 2048, transcendentals=0, bytes_accessed=8 << 20),
    )(pltpu.with_memory_space_constraint(y, pltpu.VMEM), *pieces, *([add] if which else []))


def ring_pairs(shift, first):
    pairs = []
    for z in range(4):
        for y in range(4):
            for t in range(8):
                along_y = (t % 2 == 0) == first
                to = (z, (y + shift) % 4) if along_y else ((z + shift) % 4, y)
                pairs.append(((z * 4 + y) * 8 + t, (to[0] * 4 + to[1]) * 8 + t))
    return pairs


def gather_weights(out_pool, out_attn, core):
    both = ("sp", "tp")
    half = jnp.where(core == 0, out_pool, out_attn)
    return [half] + [lax.ppermute(half, both, ring_pairs(k, True)) for k in (1, 2, 3)]


def gather_rest(line):
    both = ("sp", "tp")
    block = jnp.concatenate(line, axis=0)
    return [block] + [lax.ppermute(block, both, ring_pairs(k, False)) for k in (1, 2, 3)]


def with_partner(mine):
    swap = [(i, i ^ 1) for i in range(8)]
    return mine + [lax.ppermute(piece, "tp", swap) for piece in mine]


def body(
    inputs,
    norm_gain,
    pool_proj,
    pool_gate_proj,
    pool_mix,
    query_proj,
    key_proj,
    value_proj,
    attn_gate_proj,
    query_gain,
    key_gain,
    sink_logit,
    out_pool,
    out_attn,
):
    tp = lax.axis_index("tp")
    sp_size = lax.axis_size("sp")
    core = tp % 2
    line = gather_weights(out_pool, out_attn, core)
    head, tail, w_pool, w_attn = first_rows(
        inputs, norm_gain[None, :], pool_proj, pool_gate_proj, query_proj, key_proj.T, value_proj.T, attn_gate_proj
    )
    up = [(i, i + 1) for i in range(sp_size - 1)]
    down = [(j, i) for i, j in up]
    *line, head, tail = lax.optimization_barrier((*line, head, tail))
    before = lax.ppermute(tail, "sp", up)
    after = lax.ppermute(head, "sp", down)
    y_pool, scale = pool_branch(inputs, w_pool, pool_mix, before, after)
    *line, y_pool = lax.optimization_barrier((*line, y_pool))
    mine = gather_rest(line)
    pool_rows = lax.all_to_all(y_pool, "tp", split_axis=0, concat_axis=0, tiled=True)
    y_attn, lse = attn_branch(
        sink_logit, inputs, scale, w_attn, query_gain[None, :], key_gain[None, :], before, after
    )
    y_attn, pool_rows, *mine = lax.optimization_barrier((y_attn, pool_rows, *mine))
    pieces = with_partner(mine)
    attn_rows = lax.all_to_all(y_attn, "tp", split_axis=0, concat_axis=0, tiled=True)
    partial = half_matmul(0, pool_rows, pieces)
    mixed = half_matmul(1, attn_rows, pieces, partial)
    return mixed, jnp.transpose(lse, (2, 0, 1))


def solution(mesh):
    placed = (
        P("sp", None, None),
        P(),
        P(None, "tp"),
        P(None, "tp"),
        P("tp", None, None),
        P(None, "tp"),
        P(None, "tp"),
        P(None, "tp"),
        P(None, "tp"),
        P(),
        P(),
        P("tp"),
        P("sp", None),
        P("sp", None),
    )

    return jax.shard_map(
        body,
        mesh=mesh,
        in_specs=placed,
        out_specs=(P(("sp", "tp"), None, None), P("sp", None, "tp")),
        check_vma=False,
    )
```

```python
import functools
import math

import jax
import jax.numpy as jnp
from jax import lax
from jax.experimental import pallas as pl
from jax.experimental.pallas import tpu as pltpu
from jax.sharding import PartitionSpec as P

HEAD_DIM = 64
WINDOW = 128
REACH = 8
EPS = 1e-06
NEG = -1e30
LOG2E = math.log2(math.e)
F32 = jnp.float32
BF16 = jnp.bfloat16
BLOCK = 128


def row_scale(x):
    width = x.shape[1]
    acc = None
    for c in range(0, width, 512):
        parts = [x[:, c + d : c + d + 128] for d in range(0, 512, 128)]
        parts = [p * p for p in parts]
        four = ((parts[0] + parts[1]) + (parts[2] + parts[3])).astype(F32)
        acc = four if acc is None else acc + four
    total = jnp.sum(acc, axis=-1, keepdims=True)
    return lax.rsqrt(total * (1.0 / width) + EPS)


def silu(v):
    return v / (1.0 + jnp.exp(-v))


def first_kernel(
    x_ref, gain_ref, pool_ref, pgate_ref, query_ref, keyt_ref, valuet_ref, agate_ref,
    head_ref, tail_ref, wp_out, wa_out, w_edge, scr, xs, wp_ref, wa_ref, sems,
):
    half = x_ref.shape[0]
    step = pl.program_id(0)
    leave = [pltpu.make_async_copy(a, b, sems.at[n]) for n, (a, b) in enumerate(((wp_ref, wp_out), (wa_ref, wa_out)))]

    @pl.when(step == 0)
    def _():
        low = lax.broadcasted_iota(jnp.int32, (128, 128), 1) < HEAD_DIM
        for c in range(0, x_ref.shape[2], 128):
            rows = slice(c, c + 128)
            line = gain_ref[:, rows]
            column = jnp.broadcast_to(line, (128, 128)).T
            pool = (pool_ref[rows, :].astype(F32) * column).astype(BF16)
            wp_ref[rows, 0:128] = pool
            wp_ref[rows, 128:256] = (pgate_ref[rows, :].astype(F32) * column).astype(BF16)
            kv = (jnp.concatenate([keyt_ref[:, rows], valuet_ref[:, rows]], axis=0).astype(F32) * line).T
            turned = pltpu.roll(kv, HEAD_DIM, 1)
            wa_ref[rows, 0:128] = (query_ref[rows, :].astype(F32) * column).astype(BF16)
            wa_ref[rows, 128:256] = jnp.where(low, kv, turned).astype(BF16)
            wa_ref[rows, 256:384] = jnp.where(low, turned, kv).astype(BF16)
            wa_ref[rows, 384:512] = (agate_ref[rows, :].astype(F32) * column).astype(BF16)
            w_edge[rows, 0:128] = pool
            w_edge[rows, 128:256] = kv.astype(BF16)
        for copy in leave:
            copy.start()

    xs[...] = x_ref.reshape(half * 4, x_ref.shape[2])[...]
    x = xs[...]
    cols = jnp.dot(x, w_edge[...], preferred_element_type=F32) * row_scale(x)
    scr[0] = cols[:, :128]
    scr[1] = cols[:, 128:]
    for n in range(2):
        out = (head_ref, tail_ref)[n]

        @pl.when(step == n)
        def _(n=n, out=out):
            begin = n * 4 * (half - REACH)
            for s in range(4):
                out[s, 0:half, :] = scr[1, pl.ds(s, half, stride=4), :].astype(BF16)
                out[s, half : half + REACH, :] = scr[0, pl.ds(s + begin, REACH, stride=4), :].astype(BF16)

    @pl.when(step == 1)
    def _():
        for copy in leave:
            copy.wait()


def first_rows(x, gain, pool, pgate, query, keyt, valuet, agate):
    half = BLOCK
    width = x.shape[2]
    last = x.shape[0] // half
    whole = [gain, pool, pgate, query, keyt, valuet, agate]
    return pl.pallas_call(
        first_kernel,
        grid=(2,),
        in_specs=[pl.BlockSpec((half, 4, width), lambda i: (i * (last - 1), 0, 0))]
        + [pl.BlockSpec(a.shape, lambda i: (0, 0)) for a in whole],
        out_specs=(
            pl.BlockSpec((4, 136, 128), lambda i: (0, 0, 0)),
            pl.BlockSpec((4, 136, 128), lambda i: (0, 0, 0)),
            pl.BlockSpec(memory_space=pl.ANY),
            pl.BlockSpec(memory_space=pl.ANY),
        ),
        out_shape=(
            jax.ShapeDtypeStruct((4, 136, 128), BF16),
            jax.ShapeDtypeStruct((4, 136, 128), BF16),
            jax.ShapeDtypeStruct((width, 256), BF16),
            jax.ShapeDtypeStruct((width, 512), BF16),
        ),
        scratch_shapes=[
            pltpu.VMEM((width, 256), BF16),
            pltpu.VMEM((2, half * 4, 128), F32),
            pltpu.VMEM((half * 4, width), BF16),
            pltpu.VMEM((width, 256), BF16),
            pltpu.VMEM((width, 512), BF16),
            pltpu.SemaphoreType.DMA((2,)),
        ],
        compiler_params=pltpu.CompilerParams(dimension_semantics=("arbitrary",)),
        cost_estimate=pl.CostEstimate(flops=2 * 1024 * 2048 * 256, transcendentals=0, bytes_accessed=12 << 20),
        name="first_rows",
    )(x, *whole)


def pool_kernel(
    x_ref, w_hbm, mix_ref, before_ref, after_ref, y_hbm, scale_hbm, pool, gate, inverse, xs, xv, w_ref, yv, sv, sems, w_sem
):
    rows = BLOCK * 4
    blocks = xv.shape[0] // BLOCK
    pad = 64
    total_rows = blocks * rows
    power = lax.axis_index("tp") % 4
    half = jnp.left_shift(jnp.int32(1), power)

    def fetch(n):
        span = pl.ds(n * BLOCK, BLOCK)
        return pltpu.make_async_copy(x_ref.at[span], xv.at[span], sems.at[0, n])

    def leave(n):
        span = pl.ds(pl.multiple_of(n * rows, rows), rows)
        return (
            pltpu.make_async_copy(yv.at[n], y_hbm.at[n], sems.at[1, n]),
            pltpu.make_async_copy(sv.at[n], scale_hbm.at[span], sems.at[2, n]),
        )

    weights = pltpu.make_async_copy(w_hbm, w_ref, w_sem)
    weights.start()
    fetch(0).start()
    fetch(1).start()
    for s in range(4):
        pool[pl.ds(pad - 4 * REACH + s, REACH, stride=4), :] = before_ref[s, 128 : 128 + REACH, :].astype(F32)
        pool[pl.ds(pad + total_rows + s, REACH, stride=4), :] = after_ref[s, 128 : 128 + REACH, :].astype(F32)
    length = blocks * BLOCK
    begin = lax.axis_index("sp") * length
    total = lax.axis_size("sp") * length
    for k in range(3):
        where = (0, BLOCK, length - BLOCK)[k]
        position = begin + where + lax.broadcasted_iota(jnp.int32, (rows, 128), 0) // 4
        count = jnp.minimum(position + half - 1, total - 1) - jnp.maximum(position - half, 0) + 1
        inverse[k] = 1.0 / count.astype(F32)

    def finish(step):
        at = pl.multiple_of((step - 1) * rows, rows)
        base = pad + at
        reach = 4 * REACH
        window = pool[pl.ds(base - reach, rows + 2 * reach), :]
        size = rows + 2 * reach - 8
        two = window[:size] + window[4 : size + 4]
        four = two[: size - 8] + two[8:]
        eight = four[: size - 24] + four[16 : size - 8]
        sixteen = eight[: size - 56] + eight[32 : size - 24]
        sums = jnp.where(
            power == 0,
            two[reach - 4 : reach - 4 + rows],
            jnp.where(
                power == 1,
                four[reach - 8 : reach - 8 + rows],
                jnp.where(power == 2, eight[reach - 16 : reach - 16 + rows], sixteen[:rows]),
            ),
        )
        kind = jnp.where(step == 1, 0, jnp.where(step == blocks, 2, 1))
        pooled = (sums * inverse[kind] - window[reach : reach + rows]).astype(BF16)
        mixed = jnp.dot(pooled, mix_ref[0], preferred_element_type=F32)
        yv[step - 1] = (mixed * silu(gate[pl.ds(at, rows), :])).astype(BF16)
        for copy in leave(step - 1):
            copy.start()

    def project(step):
        fetch(step).wait()

        @pl.when(step + 2 < blocks)
        def _():
            fetch(step + 2).start()

        xs[...] = xv.at[pl.ds(pl.multiple_of(step * BLOCK, BLOCK), BLOCK)].reshape(rows, xv.shape[2])[...]
        x = xs[...]
        scale = row_scale(x)
        sv[step] = jnp.broadcast_to(scale, (rows, 128))
        both = jnp.dot(x, w_ref[...], preferred_element_type=F32) * scale
        at = pl.multiple_of(step * rows, rows)
        pool[pl.ds(pad + at, rows), :] = both[:, :128]
        gate[pl.ds(at, rows), :] = both[:, 128:]

    weights.wait()
    project(0)

    @pl.loop(1, blocks)
    def _(step):
        project(step)
        finish(step)

    finish(blocks)
    for n in range(blocks):
        for copy in leave(n):
            copy.wait()


def pool_branch(x, w, mix, before, after):
    length, _, width = x.shape
    blocks = length // BLOCK
    rows = BLOCK * 4
    whole = pl.BlockSpec(memory_space=pltpu.VMEM)
    far = pl.BlockSpec(memory_space=pl.ANY)
    return pl.pallas_call(
        pool_kernel,
        in_specs=[far, far, whole, whole, whole],
        out_specs=(far, far),
        out_shape=(
            jax.ShapeDtypeStruct((blocks, rows, 128), BF16),
            jax.ShapeDtypeStruct((length * 4, 128), F32),
        ),
        scratch_shapes=[
            pltpu.VMEM((length * 4 + 128, 128), F32),
            pltpu.VMEM((length * 4, 128), F32),
            pltpu.VMEM((3, rows, 128), F32),
            pltpu.VMEM((rows, width), BF16),
            pltpu.VMEM(x.shape, BF16),
            pltpu.VMEM(w.shape, BF16),
            pltpu.VMEM((blocks, rows, 128), BF16),
            pltpu.VMEM((blocks, rows, 128), F32),
            pltpu.SemaphoreType.DMA((3, blocks)),
            pltpu.SemaphoreType.DMA,
        ],
        cost_estimate=pl.CostEstimate(flops=2 * 4096 * 2048 * 256, transcendentals=0, bytes_accessed=18 << 20),
        name="pool_branch",
    )(x, w, mix, before, after)


def attn_kernel(
    sink_ref, x_ref, scale_ref, w_ref, qgain_ref, kgain_ref, before_ref, after_ref,
    y_ref, lse_ref, proj, qs, ks, vs, gate, bias, att, xs, sinks, gains, same,
):
    step = pl.program_id(0)
    blocks = pl.num_programs(0) - 1
    rows = BLOCK * 4
    lane = lax.broadcasted_iota(jnp.int32, (BLOCK, 128), 1)
    low_lanes = lane < HEAD_DIM
    shifts = [jnp.maximum(sink_ref[h], 0.0) for h in range(2)]

    @pl.when(step == 0)
    def _():
        query = lax.broadcasted_iota(jnp.int32, (BLOCK, 3 * BLOCK), 0)
        key = lax.broadcasted_iota(jnp.int32, (BLOCK, 3 * BLOCK), 1) - BLOCK
        distance = jnp.abs(query - key)
        r = lax.broadcasted_iota(jnp.int32, (256, 256), 0) // HEAD_DIM
        c = lax.broadcasted_iota(jnp.int32, (256, 256), 1) // HEAD_DIM
        same[...] = jnp.where(r == c, 1.0, 0.0).astype(BF16)
        scale = lax.broadcasted_iota(jnp.int32, (BLOCK, 3 * BLOCK), 0) * 0 + jnp.left_shift(
            jnp.int32(1), lax.axis_index("tp")
        )
        for h in range(2):
            slope = ((0.5**0.5, 0.5)[h] * LOG2E) / scale.astype(F32)
            line = -slope * distance.astype(F32) - shifts[h] * LOG2E
            bias[h * BLOCK : (h + 1) * BLOCK, :] = jnp.where(distance <= WINDOW, line, NEG)
        shift_row = jnp.where(low_lanes, shifts[0], shifts[1])
        sink_row = jnp.where(low_lanes, sink_ref[0], sink_ref[1])
        sinks[...] = jnp.exp(sink_row - shift_row)
        qgain = qgain_ref[...] * (LOG2E * HEAD_DIM**-0.5)
        gains[...] = jnp.concatenate([qgain, qgain, kgain_ref[...], kgain_ref[...]], axis=1)
        key_gain = jnp.concatenate([kgain_ref[...], kgain_ref[...]], axis=1)
        sp = lax.axis_index("sp")
        for side, ref in enumerate((before_ref, after_ref)):
            at = 0 if side == 0 else (blocks + 1) * BLOCK
            live = (sp > 0) if side == 0 else (sp < lax.axis_size("sp") - 1)
            live = jnp.where(live, 1.0, 0.0)
            for s in range(4):
                kv = ref[s, 0:128, :].astype(F32)
                turned = pltpu.roll(kv, HEAD_DIM, 1)
                kk = jnp.where(low_lanes, kv, turned)
                vv = jnp.where(low_lanes, turned, kv)
                mean = jnp.sum(jnp.where(low_lanes, kv * kv, 0.0), axis=-1, keepdims=True) * (1.0 / HEAD_DIM)
                ks[s, pl.ds(at, BLOCK), :] = (kk * lax.rsqrt(mean + EPS) * key_gain).astype(BF16)
                vs[s, pl.ds(at, BLOCK), 0:128] = vv.astype(BF16)
                vs[s, pl.ds(at, BLOCK), 128:256] = jnp.full((BLOCK, 128), live, F32).astype(BF16)

    def project(part):
        size = rows // 2
        at = part * size
        xs[at : at + size, :] = x_ref.at[part * (BLOCK // 2) : (part + 1) * (BLOCK // 2)].reshape(size, x_ref.shape[2])[...]
        x = xs[at : at + size, :]
        cols = jnp.dot(x, w_ref[...], preferred_element_type=F32)
        scale = scale_ref[at : at + size, :]
        qk = cols[:, :256] * jnp.concatenate([scale, scale], axis=1)
        squares = jnp.dot((qk * qk).astype(BF16), same[...], preferred_element_type=F32)
        normed = qk * lax.rsqrt(squares * (1.0 / HEAD_DIM) + EPS) * gains[...]
        proj[0, at : at + size] = normed[:, :128]
        proj[1, at : at + size] = normed[:, 128:]
        proj[2, at : at + size] = cols[:, 256:384] * scale
        gate[step % 2, at : at + size, :] = cols[:, 384:] * scale

    def separate():
        at = pl.multiple_of(step * BLOCK, BLOCK)
        for s in range(4):
            mine = pl.ds(s, BLOCK, stride=4)
            qs[step % 2, s] = proj[0, mine, :].astype(BF16)
            ks[s, pl.ds(at + BLOCK, BLOCK), :] = proj[1, mine, :].astype(BF16)
            vs[s, pl.ds(at + BLOCK, BLOCK), 0:128] = proj[2, mine, :].astype(BF16)
            vs[s, pl.ds(at + BLOCK, BLOCK), 128:256] = jnp.ones((BLOCK, 128), BF16)

    def attend(s):
        at = pl.multiple_of((step - 1) * BLOCK, BLOCK)
        q = qs[(step - 1) % 2, s]
        zero = jnp.zeros_like(q)
        two = jnp.concatenate([jnp.where(low_lanes, q, zero), jnp.where(low_lanes, zero, q)], axis=0)
        keys = ks[s, pl.ds(at, 3 * BLOCK), :]
        score = lax.dot_general(two, keys, (((1,), (1,)), ((), ())), preferred_element_type=F32)
        weight = jnp.exp2(score + bias[...]).astype(BF16)
        out = jnp.dot(weight, vs[s, pl.ds(at, 3 * BLOCK), :], preferred_element_type=F32)
        total = jnp.where(low_lanes, out[:BLOCK, 128:], out[BLOCK:, 128:]) + sinks[...]
        value = jnp.where(low_lanes, out[:BLOCK, :128], out[BLOCK:, :128])
        att[pl.ds(s, BLOCK, stride=4), :] = value / total
        turned = total.T
        lse_ref[s, 0:1, :] = jnp.log(turned[0:1, :]) + shifts[0]
        lse_ref[s, 1:2, :] = jnp.log(turned[HEAD_DIM : HEAD_DIM + 1, :]) + shifts[1]

    def close():
        y_ref[0] = (att[...] * silu(gate[(step - 1) % 2])).astype(BF16)

    @pl.when(step < blocks)
    def _():
        project(0)
        project(1)
        separate()

    @pl.when(step > 0)
    def _():
        for s in range(4):
            attend(s)
        close()


def attn_branch(sink, x, scale, w, qgain, kgain, before, after):
    length, _, width = x.shape
    blocks = length // BLOCK
    rows = BLOCK * 4
    return pl.pallas_call(
        attn_kernel,
        grid=(blocks + 1,),
        in_specs=[
            pl.BlockSpec(memory_space=pltpu.SMEM),
            pl.BlockSpec((BLOCK, 4, width), lambda i: (jnp.minimum(i, blocks - 1), 0, 0)),
            pl.BlockSpec((rows, 128), lambda i: (jnp.minimum(i, blocks - 1), 0)),
            pl.BlockSpec(w.shape, lambda i: (0, 0)),
            pl.BlockSpec(qgain.shape, lambda i: (0, 0)),
            pl.BlockSpec(kgain.shape, lambda i: (0, 0)),
            pl.BlockSpec(before.shape, lambda i: (0, 0, 0)),
            pl.BlockSpec(after.shape, lambda i: (0, 0, 0)),
        ],
        out_specs=(
            pl.BlockSpec((1, rows, 128), lambda i: (jnp.maximum(i - 1, 0), 0, 0)),
            pl.BlockSpec((4, 2, BLOCK), lambda i: (0, 0, jnp.maximum(i - 1, 0))),
        ),
        out_shape=(
            jax.ShapeDtypeStruct((blocks, rows, 128), BF16),
            jax.ShapeDtypeStruct((4, 2, length), F32),
        ),
        scratch_shapes=[
            pltpu.VMEM((3, rows, 128), F32),
            pltpu.VMEM((2, 4, BLOCK, 128), BF16),
            pltpu.VMEM((4, length + 2 * BLOCK, 128), BF16),
            pltpu.VMEM((4, length + 2 * BLOCK, 256), BF16),
            pltpu.VMEM((2, rows, 128), F32),
            pltpu.VMEM((2 * BLOCK, 3 * BLOCK), F32),
            pltpu.VMEM((rows, 128), F32),
            pltpu.VMEM((rows, width), BF16),
            pltpu.VMEM((BLOCK, 128), F32),
            pltpu.VMEM((1, 256), F32),
            pltpu.VMEM((256, 256), BF16),
        ],
        compiler_params=pltpu.CompilerParams(dimension_semantics=("arbitrary",)),
        cost_estimate=pl.CostEstimate(flops=2 * 4096 * 2048 * 768, transcendentals=3 << 20, bytes_accessed=20 << 20),
        name="attn_branch",
    )(sink, x, scale, w, qgain, kgain, before, after)


def half_kernel(which, y_ref, *rest):
    pieces, rest = rest[:8], rest[8:]
    add_ref, (o_ref, w, sems) = (None, rest) if which == 0 else (rest[0], rest[1:])
    tiles, _, tile = w.shape
    rows = y_ref.shape[1]
    step = pl.program_id(0)
    place = lax.axis_index("sp")
    z, y, core = place // 4, place % 4, lax.axis_index("tp") % 2

    def copies(n, side):
        for m in range(4):
            for k in range(4):
                a = (z + 4 - (m if which == 0 else k)) % 4
                b = (y + 4 - (k if which == 0 else m)) % 4
                row = pl.multiple_of((a * 4 + b) * 64, 64)
                yield pltpu.make_async_copy(
                    pieces[side * 4 + m].at[pl.ds(k * 64, 64), pl.ds(n * tile, tile)],
                    w.at[n, pl.ds(row, 64), :],
                    sems.at[n, m * 4 + k],
                )

    for side in range(2):

        @pl.when((step == 0) & (core == (which if side == 0 else 1 - which)))
        def _(side=side):
            for n in range(tiles):
                for copy in copies(n, side):
                    copy.start()

    for n in range(tiles):

        @pl.when(step == n)
        def _(n=n):
            for copy in copies(n, 0):
                copy.wait()

    lanes = jnp.concatenate([y_ref[j] for j in range(y_ref.shape[0])], axis=1)
    acc = jnp.dot(lanes, w[step], preferred_element_type=F32)
    if which == 0:
        o_ref[...] = acc.astype(BF16)
    else:
        o_ref.reshape(rows, tile)[...] = (acc + add_ref[...].astype(F32)).astype(BF16)


def half_matmul(which, y, pieces, add=None):
    parts, rows, cols = y.shape
    width = pieces[0].shape[1]
    tile = 1024
    steps = width // tile
    if which == 0:
        out_spec = pl.BlockSpec((rows, tile), lambda n: (0, n))
        out_shape = jax.ShapeDtypeStruct((rows, width), BF16)
    else:
        out_spec = pl.BlockSpec((rows // 4, 4, tile), lambda n: (0, 0, n))
        out_shape = jax.ShapeDtypeStruct((rows // 4, 4, width), BF16)
    return pl.pallas_call(
        functools.partial(half_kernel, which),
        grid=(steps,),
        in_specs=[pl.BlockSpec(memory_space=pltpu.VMEM)]
        + [pl.BlockSpec(memory_space=pl.ANY)] * 8
        + ([pl.BlockSpec((rows, tile), lambda n: (0, n))] if which else []),
        out_specs=out_spec,
        out_shape=out_shape,
        scratch_shapes=[
            pltpu.VMEM((steps, parts * cols, tile), BF16),
            pltpu.SemaphoreType.DMA((steps, 16)),
        ],
        compiler_params=pltpu.CompilerParams(dimension_semantics=("arbitrary",)),
        cost_estimate=pl.CostEstimate(flops=512 * 2048 * 2048, transcendentals=0, bytes_accessed=8 << 20),
    )(pltpu.with_memory_space_constraint(y, pltpu.VMEM), *pieces, *([add] if which else []))


def ring_pairs(shift, first):
    pairs = []
    for z in range(4):
        for y in range(4):
            for t in range(8):
                along_y = (t % 2 == 0) == first
                to = (z, (y + shift) % 4) if along_y else ((z + shift) % 4, y)
                pairs.append(((z * 4 + y) * 8 + t, (to[0] * 4 + to[1]) * 8 + t))
    return pairs


def gather_weights(out_pool, out_attn, core):
    both = ("sp", "tp")
    half = jnp.where(core == 0, out_pool, out_attn)
    return [half] + [lax.ppermute(half, both, ring_pairs(k, True)) for k in (1, 2, 3)]


def gather_rest(line):
    both = ("sp", "tp")
    block = jnp.concatenate(line, axis=0)
    return [block] + [lax.ppermute(block, both, ring_pairs(k, False)) for k in (1, 2, 3)]


def with_partner(mine):
    swap = [(i, i ^ 1) for i in range(8)]
    return mine + [lax.ppermute(piece, "tp", swap) for piece in mine]


def body(
    inputs,
    norm_gain,
    pool_proj,
    pool_gate_proj,
    pool_mix,
    query_proj,
    key_proj,
    value_proj,
    attn_gate_proj,
    query_gain,
    key_gain,
    sink_logit,
    out_pool,
    out_attn,
):
    tp = lax.axis_index("tp")
    sp_size = lax.axis_size("sp")
    core = tp % 2
    line = gather_weights(out_pool, out_attn, core)
    head, tail, w_pool, w_attn = first_rows(
        inputs, norm_gain[None, :], pool_proj, pool_gate_proj, query_proj, key_proj.T, value_proj.T, attn_gate_proj
    )
    up = [(i, i + 1) for i in range(sp_size - 1)]
    down = [(j, i) for i, j in up]
    *line, head, tail = lax.optimization_barrier((*line, head, tail))
    before = lax.ppermute(tail, "sp", up)
    after = lax.ppermute(head, "sp", down)
    y_pool, scale = pool_branch(inputs, w_pool, pool_mix, before, after)
    *line, y_pool = lax.optimization_barrier((*line, y_pool))
    mine = gather_rest(line)
    pool_rows = lax.all_to_all(y_pool, "tp", split_axis=0, concat_axis=0, tiled=True)
    y_attn, lse = attn_branch(
        sink_logit, inputs, scale, w_attn, query_gain[None, :], key_gain[None, :], before, after
    )
    y_attn, pool_rows, *mine = lax.optimization_barrier((y_attn, pool_rows, *mine))
    pieces = with_partner(mine)
    attn_rows = lax.all_to_all(y_attn, "tp", split_axis=0, concat_axis=0, tiled=True)
    partial = half_matmul(0, pool_rows, pieces)
    mixed = half_matmul(1, attn_rows, pieces, partial)
    return mixed, jnp.transpose(lse, (2, 0, 1))


def solution(mesh):
    placed = (
        P("sp", None, None),
        P(),
        P(None, "tp"),
        P(None, "tp"),
        P("tp", None, None),
        P(None, "tp"),
        P(None, "tp"),
        P(None, "tp"),
        P(None, "tp"),
        P(),
        P(),
        P("tp"),
        P("sp", None),
        P("sp", None),
    )

    return jax.shard_map(
        body,
        mesh=mesh,
        in_specs=placed,
        out_specs=(P(("sp", "tp"), None, None), P("sp", None, "tp")),
        check_vma=False,
    )
```

```python
import functools
import math

import jax
import jax.numpy as jnp
from jax import lax
from jax.experimental import pallas as pl
from jax.experimental.pallas import tpu as pltpu
from jax.sharding import PartitionSpec as P


HEAD_DIM = 64
WINDOW = 128
REACH = 8
EPS = 1e-06
NEG = -1e30
LOG2E = math.log2(math.e)
F32 = jnp.float32
BF16 = jnp.bfloat16
BLOCK = 128


def row_scale(x):
    width = x.shape[1]
    acc = None
    for c in range(0, width, 512):
        parts = [x[:, c + d : c + d + 128] for d in range(0, 512, 128)]
        parts = [p * p for p in parts]
        four = ((parts[0] + parts[1]) + (parts[2] + parts[3])).astype(F32)
        acc = four if acc is None else acc + four
    total = jnp.sum(acc, axis=-1, keepdims=True)
    return lax.rsqrt(total * (1.0 / width) + EPS)


def silu(v):
    return v / (1.0 + jnp.exp(-v))


def first_kernel(
    x_ref, gain_ref, pool_ref, pgate_ref, query_ref, keyt_ref, valuet_ref, agate_ref,
    head_ref, tail_ref, wp_out, wa_out, w_edge, scr, xs, wp_ref, wa_ref, sems,
):
    half = x_ref.shape[0]
    step = pl.program_id(0)
    leave = [pltpu.make_async_copy(a, b, sems.at[n]) for n, (a, b) in enumerate(((wp_ref, wp_out), (wa_ref, wa_out)))]

    @pl.when(step == 0)
    def _():
        low = lax.broadcasted_iota(jnp.int32, (128, 128), 1) < HEAD_DIM
        for c in range(0, x_ref.shape[2], 128):
            rows = slice(c, c + 128)
            line = gain_ref[:, rows]
            column = jnp.broadcast_to(line, (128, 128)).T
            pool = (pool_ref[rows, :].astype(F32) * column).astype(BF16)
            wp_ref[rows, 0:128] = pool
            wp_ref[rows, 128:256] = (pgate_ref[rows, :].astype(F32) * column).astype(BF16)
            kv = (jnp.concatenate([keyt_ref[:, rows], valuet_ref[:, rows]], axis=0).astype(F32) * line).T
            turned = pltpu.roll(kv, HEAD_DIM, 1)
            wa_ref[rows, 0:128] = (query_ref[rows, :].astype(F32) * column).astype(BF16)
            wa_ref[rows, 128:256] = jnp.where(low, kv, turned).astype(BF16)
            wa_ref[rows, 256:384] = jnp.where(low, turned, kv).astype(BF16)
            wa_ref[rows, 384:512] = (agate_ref[rows, :].astype(F32) * column).astype(BF16)
            w_edge[rows, 0:128] = pool
            w_edge[rows, 128:256] = kv.astype(BF16)
        for copy in leave:
            copy.start()

    xs[...] = x_ref.reshape(half * 4, x_ref.shape[2])[...]
    x = xs[...]
    cols = jnp.dot(x, w_edge[...], preferred_element_type=F32) * row_scale(x)
    scr[0] = cols[:, :128]
    scr[1] = cols[:, 128:]
    for n in range(2):
        out = (head_ref, tail_ref)[n]

        @pl.when(step == n)
        def _(n=n, out=out):
            begin = n * 4 * (half - REACH)
            for s in range(4):
                out[s, 0:half, :] = scr[1, pl.ds(s, half, stride=4), :].astype(BF16)
                out[s, half : half + REACH, :] = scr[0, pl.ds(s + begin, REACH, stride=4), :].astype(BF16)

    @pl.when(step == 1)
    def _():
        for copy in leave:
            copy.wait()


def first_rows(x, gain, pool, pgate, query, keyt, valuet, agate):
    half = BLOCK
    width = x.shape[2]
    last = x.shape[0] // half
    whole = [gain, pool, pgate, query, keyt, valuet, agate]
    return pl.pallas_call(
        first_kernel,
        grid=(2,),
        in_specs=[pl.BlockSpec((half, 4, width), lambda i: (i * (last - 1), 0, 0))]
        + [pl.BlockSpec(a.shape, lambda i: (0, 0)) for a in whole],
        out_specs=(
            pl.BlockSpec((4, 136, 128), lambda i: (0, 0, 0)),
            pl.BlockSpec((4, 136, 128), lambda i: (0, 0, 0)),
            pl.BlockSpec(memory_space=pl.ANY),
            pl.BlockSpec(memory_space=pl.ANY),
        ),
        out_shape=(
            jax.ShapeDtypeStruct((4, 136, 128), BF16),
            jax.ShapeDtypeStruct((4, 136, 128), BF16),
            jax.ShapeDtypeStruct((width, 256), BF16),
            jax.ShapeDtypeStruct((width, 512), BF16),
        ),
        scratch_shapes=[
            pltpu.VMEM((width, 256), BF16),
            pltpu.VMEM((2, half * 4, 128), F32),
            pltpu.VMEM((half * 4, width), BF16),
            pltpu.VMEM((width, 256), BF16),
            pltpu.VMEM((width, 512), BF16),
            pltpu.SemaphoreType.DMA((2,)),
        ],
        compiler_params=pltpu.CompilerParams(dimension_semantics=("arbitrary",)),
        cost_estimate=pl.CostEstimate(flops=2 * 1024 * 2048 * 256, transcendentals=0, bytes_accessed=12 << 20),
        name="first_rows",
    )(x, *whole)


def pool_kernel(
    x_ref, w_hbm, mix_ref, before_ref, after_ref, y_hbm, scale_hbm, pool, gate, inverse, xs, xv, w_ref, yv, sv, sems, w_sem
):
    rows = BLOCK * 4
    blocks = xv.shape[0] // BLOCK
    pad = 64
    total_rows = blocks * rows
    power = lax.axis_index("tp") % 4
    half = jnp.left_shift(jnp.int32(1), power)

    def fetch(n):
        span = pl.ds(n * BLOCK, BLOCK)
        return pltpu.make_async_copy(x_ref.at[span], xv.at[span], sems.at[0, n])

    def leave(n):
        span = pl.ds(pl.multiple_of(n * rows, rows), rows)
        return (
            pltpu.make_async_copy(yv.at[n], y_hbm.at[n], sems.at[1, n]),
            pltpu.make_async_copy(sv.at[n], scale_hbm.at[span], sems.at[2, n]),
        )

    weights = pltpu.make_async_copy(w_hbm, w_ref, w_sem)
    weights.start()
    fetch(0).start()
    fetch(1).start()
    for s in range(4):
        pool[pl.ds(pad - 4 * REACH + s, REACH, stride=4), :] = before_ref[s, 128 : 128 + REACH, :].astype(F32)
        pool[pl.ds(pad + total_rows + s, REACH, stride=4), :] = after_ref[s, 128 : 128 + REACH, :].astype(F32)
    length = blocks * BLOCK
    begin = lax.axis_index("sp") * length
    total = lax.axis_size("sp") * length
    for k in range(3):
        where = (0, BLOCK, length - BLOCK)[k]
        position = begin + where + lax.broadcasted_iota(jnp.int32, (rows, 128), 0) // 4
        count = jnp.minimum(position + half - 1, total - 1) - jnp.maximum(position - half, 0) + 1
        inverse[k] = 1.0 / count.astype(F32)

    def finish(step):
        at = pl.multiple_of((step - 1) * rows, rows)
        base = pad + at
        reach = 4 * REACH
        window = pool[pl.ds(base - reach, rows + 2 * reach), :]
        size = rows + 2 * reach - 8
        two = window[:size] + window[4 : size + 4]
        four = two[: size - 8] + two[8:]
        eight = four[: size - 24] + four[16 : size - 8]
        sixteen = eight[: size - 56] + eight[32 : size - 24]
        sums = jnp.where(
            power == 0,
            two[reach - 4 : reach - 4 + rows],
            jnp.where(
                power == 1,
                four[reach - 8 : reach - 8 + rows],
                jnp.where(power == 2, eight[reach - 16 : reach - 16 + rows], sixteen[:rows]),
            ),
        )
        kind = jnp.where(step == 1, 0, jnp.where(step == blocks, 2, 1))
        pooled = (sums * inverse[kind] - window[reach : reach + rows]).astype(BF16)
        mixed = jnp.dot(pooled, mix_ref[0], preferred_element_type=F32)
        yv[step - 1] = (mixed * silu(gate[pl.ds(at, rows), :])).astype(BF16)
        for copy in leave(step - 1):
            copy.start()

    def project(step):
        fetch(step).wait()

        @pl.when(step + 2 < blocks)
        def _():
            fetch(step + 2).start()

        xs[...] = xv.at[pl.ds(pl.multiple_of(step * BLOCK, BLOCK), BLOCK)].reshape(rows, xv.shape[2])[...]
        x = xs[...]
        scale = row_scale(x)
        sv[step] = jnp.broadcast_to(scale, (rows, 128))
        both = jnp.dot(x, w_ref[...], preferred_element_type=F32) * scale
        at = pl.multiple_of(step * rows, rows)
        pool[pl.ds(pad + at, rows), :] = both[:, :128]
        gate[pl.ds(at, rows), :] = both[:, 128:]

    weights.wait()
    project(0)

    @pl.loop(1, blocks)
    def _(step):
        project(step)
        finish(step)

    finish(blocks)
    for n in range(blocks):
        for copy in leave(n):
            copy.wait()


def pool_branch(x, w, mix, before, after):
    length, _, width = x.shape
    blocks = length // BLOCK
    rows = BLOCK * 4
    whole = pl.BlockSpec(memory_space=pltpu.VMEM)
    far = pl.BlockSpec(memory_space=pl.ANY)
    return pl.pallas_call(
        pool_kernel,
        in_specs=[far, far, whole, whole, whole],
        out_specs=(far, far),
        out_shape=(
            jax.ShapeDtypeStruct((blocks, rows, 128), BF16),
            jax.ShapeDtypeStruct((length * 4, 128), F32),
        ),
        scratch_shapes=[
            pltpu.VMEM((length * 4 + 128, 128), F32),
            pltpu.VMEM((length * 4, 128), F32),
            pltpu.VMEM((3, rows, 128), F32),
            pltpu.VMEM((rows, width), BF16),
            pltpu.VMEM(x.shape, BF16),
            pltpu.VMEM(w.shape, BF16),
            pltpu.VMEM((blocks, rows, 128), BF16),
            pltpu.VMEM((blocks, rows, 128), F32),
            pltpu.SemaphoreType.DMA((3, blocks)),
            pltpu.SemaphoreType.DMA,
        ],
        cost_estimate=pl.CostEstimate(flops=2 * 4096 * 2048 * 256, transcendentals=0, bytes_accessed=18 << 20),
        name="pool_branch",
    )(x, w, mix, before, after)


def attn_kernel(
    sink_ref, x_ref, scale_ref, w_ref, qgain_ref, kgain_ref, before_ref, after_ref,
    y_ref, lse_ref, proj, qs, ks, vs, gate, bias, att, xs, sinks, gains, same,
):
    step = pl.program_id(0)
    blocks = pl.num_programs(0) - 1
    rows = BLOCK * 4
    lane = lax.broadcasted_iota(jnp.int32, (BLOCK, 128), 1)
    low_lanes = lane < HEAD_DIM
    shifts = [jnp.maximum(sink_ref[h], 0.0) for h in range(2)]

    @pl.when(step == 0)
    def _():
        query = lax.broadcasted_iota(jnp.int32, (BLOCK, 3 * BLOCK), 0)
        key = lax.broadcasted_iota(jnp.int32, (BLOCK, 3 * BLOCK), 1) - BLOCK
        distance = jnp.abs(query - key)
        r = lax.broadcasted_iota(jnp.int32, (256, 256), 0) // HEAD_DIM
        c = lax.broadcasted_iota(jnp.int32, (256, 256), 1) // HEAD_DIM
        same[...] = jnp.where(r == c, 1.0, 0.0).astype(BF16)
        scale = lax.broadcasted_iota(jnp.int32, (BLOCK, 3 * BLOCK), 0) * 0 + jnp.left_shift(
            jnp.int32(1), lax.axis_index("tp")
        )
        for h in range(2):
            slope = ((0.5**0.5, 0.5)[h] * LOG2E) / scale.astype(F32)
            line = -slope * distance.astype(F32) - shifts[h] * LOG2E
            bias[h * BLOCK : (h + 1) * BLOCK, :] = jnp.where(distance <= WINDOW, line, NEG)
        shift_row = jnp.where(low_lanes, shifts[0], shifts[1])
        sink_row = jnp.where(low_lanes, sink_ref[0], sink_ref[1])
        sinks[...] = jnp.exp(sink_row - shift_row)
        qgain = qgain_ref[...] * (LOG2E * HEAD_DIM**-0.5)
        gains[...] = jnp.concatenate([qgain, qgain, kgain_ref[...], kgain_ref[...]], axis=1)
        key_gain = jnp.concatenate([kgain_ref[...], kgain_ref[...]], axis=1)
        sp = lax.axis_index("sp")
        for side, ref in enumerate((before_ref, after_ref)):
            at = 0 if side == 0 else (blocks + 1) * BLOCK
            live = (sp > 0) if side == 0 else (sp < lax.axis_size("sp") - 1)
            live = jnp.where(live, 1.0, 0.0)
            for s in range(4):
                kv = ref[s, 0:128, :].astype(F32)
                turned = pltpu.roll(kv, HEAD_DIM, 1)
                kk = jnp.where(low_lanes, kv, turned)
                vv = jnp.where(low_lanes, turned, kv)
                mean = jnp.sum(jnp.where(low_lanes, kv * kv, 0.0), axis=-1, keepdims=True) * (1.0 / HEAD_DIM)
                ks[s, pl.ds(at, BLOCK), :] = (kk * lax.rsqrt(mean + EPS) * key_gain).astype(BF16)
                vs[s, pl.ds(at, BLOCK), 0:128] = vv.astype(BF16)
                vs[s, pl.ds(at, BLOCK), 128:256] = jnp.full((BLOCK, 128), live, F32).astype(BF16)

    def project():
        size, at = rows, 0
        xs[...] = x_ref.reshape(rows, x_ref.shape[2])[...]
        x = xs[...]
        cols = jnp.dot(x, w_ref[...], preferred_element_type=F32)
        scale = scale_ref[at : at + size, :]
        qk = cols[:, :256] * jnp.concatenate([scale, scale], axis=1)
        squares = jnp.dot((qk * qk).astype(BF16), same[...], preferred_element_type=F32)
        normed = qk * lax.rsqrt(squares * (1.0 / HEAD_DIM) + EPS) * gains[...]
        proj[0, at : at + size] = normed[:, :128]
        proj[1, at : at + size] = normed[:, 128:]
        proj[2, at : at + size] = cols[:, 256:384] * scale
        gate[step % 2, at : at + size, :] = cols[:, 384:] * scale

    def separate():
        at = pl.multiple_of(step * BLOCK, BLOCK)
        for s in range(4):
            mine = pl.ds(s, BLOCK, stride=4)
            qs[step % 2, s] = proj[0, mine, :].astype(BF16)
            ks[s, pl.ds(at + BLOCK, BLOCK), :] = proj[1, mine, :].astype(BF16)
            vs[s, pl.ds(at + BLOCK, BLOCK), 0:128] = proj[2, mine, :].astype(BF16)
            vs[s, pl.ds(at + BLOCK, BLOCK), 128:256] = jnp.ones((BLOCK, 128), BF16)

    def attend(s):
        at = pl.multiple_of((step - 1) * BLOCK, BLOCK)
        q = qs[(step - 1) % 2, s]
        zero = jnp.zeros_like(q)
        two = jnp.concatenate([jnp.where(low_lanes, q, zero), jnp.where(low_lanes, zero, q)], axis=0)
        keys = ks[s, pl.ds(at, 3 * BLOCK), :]
        score = lax.dot_general(two, keys, (((1,), (1,)), ((), ())), preferred_element_type=F32)
        weight = jnp.exp2(score + bias[...]).astype(BF16)
        out = jnp.dot(weight, vs[s, pl.ds(at, 3 * BLOCK), :], preferred_element_type=F32)
        total = jnp.where(low_lanes, out[:BLOCK, 128:], out[BLOCK:, 128:]) + sinks[...]
        value = jnp.where(low_lanes, out[:BLOCK, :128], out[BLOCK:, :128])
        att[pl.ds(s, BLOCK, stride=4), :] = value / total
        turned = total.T
        lse_ref[s, 0:1, :] = jnp.log(turned[0:1, :]) + shifts[0]
        lse_ref[s, 1:2, :] = jnp.log(turned[HEAD_DIM : HEAD_DIM + 1, :]) + shifts[1]

    def close():
        y_ref[0] = (att[...] * silu(gate[(step - 1) % 2])).astype(BF16)

    @pl.when(step < blocks)
    def _():
        project()
        separate()

    @pl.when(step > 0)
    def _():
        for s in range(4):
            attend(s)
        close()


def attn_branch(sink, x, scale, w, qgain, kgain, before, after):
    length, _, width = x.shape
    blocks = length // BLOCK
    rows = BLOCK * 4
    return pl.pallas_call(
        attn_kernel,
        grid=(blocks + 1,),
        in_specs=[
            pl.BlockSpec(memory_space=pltpu.SMEM),
            pl.BlockSpec((BLOCK, 4, width), lambda i: (jnp.minimum(i, blocks - 1), 0, 0)),
            pl.BlockSpec((rows, 128), lambda i: (jnp.minimum(i, blocks - 1), 0)),
            pl.BlockSpec(w.shape, lambda i: (0, 0)),
            pl.BlockSpec(qgain.shape, lambda i: (0, 0)),
            pl.BlockSpec(kgain.shape, lambda i: (0, 0)),
            pl.BlockSpec(before.shape, lambda i: (0, 0, 0)),
            pl.BlockSpec(after.shape, lambda i: (0, 0, 0)),
        ],
        out_specs=(
            pl.BlockSpec((1, rows, 128), lambda i: (jnp.maximum(i - 1, 0), 0, 0)),
            pl.BlockSpec((4, 2, BLOCK), lambda i: (0, 0, jnp.maximum(i - 1, 0))),
        ),
        out_shape=(
            jax.ShapeDtypeStruct((blocks, rows, 128), BF16),
            jax.ShapeDtypeStruct((4, 2, length), F32),
        ),
        scratch_shapes=[
            pltpu.VMEM((3, rows, 128), F32),
            pltpu.VMEM((2, 4, BLOCK, 128), BF16),
            pltpu.VMEM((4, length + 2 * BLOCK, 128), BF16),
            pltpu.VMEM((4, length + 2 * BLOCK, 256), BF16),
            pltpu.VMEM((2, rows, 128), F32),
            pltpu.VMEM((2 * BLOCK, 3 * BLOCK), F32),
            pltpu.VMEM((rows, 128), F32),
            pltpu.VMEM((rows, width), BF16),
            pltpu.VMEM((BLOCK, 128), F32),
            pltpu.VMEM((1, 256), F32),
            pltpu.VMEM((256, 256), BF16),
        ],
        compiler_params=pltpu.CompilerParams(dimension_semantics=("arbitrary",)),
        cost_estimate=pl.CostEstimate(flops=2 * 4096 * 2048 * 768, transcendentals=3 << 20, bytes_accessed=20 << 20),
        name="attn_branch",
    )(sink, x, scale, w, qgain, kgain, before, after)


def half_kernel(which, y_ref, *rest):
    pieces, rest = rest[:8], rest[8:]
    add_ref, (o_ref, w, sems) = (None, rest) if which == 0 else (rest[0], rest[1:])
    tiles, _, tile = w.shape
    rows = y_ref.shape[1]
    step = pl.program_id(0)
    place = lax.axis_index("sp")
    z, y, core = place // 4, place % 4, lax.axis_index("tp") % 2

    def copies(n, side):
        for m in range(4):
            for k in range(4):
                a = (z + 4 - (m if which == 0 else k)) % 4
                b = (y + 4 - (k if which == 0 else m)) % 4
                row = pl.multiple_of((a * 4 + b) * 64, 64)
                yield pltpu.make_async_copy(
                    pieces[side * 4 + m].at[pl.ds(k * 64, 64), pl.ds(n * tile, tile)],
                    w.at[n, pl.ds(row, 64), :],
                    sems.at[n, m * 4 + k],
                )

    for side in range(2):

        @pl.when((step == 0) & (core == (which if side == 0 else 1 - which)))
        def _(side=side):
            for n in range(tiles):
                for copy in copies(n, side):
                    copy.start()

    for n in range(tiles):

        @pl.when(step == n)
        def _(n=n):
            for copy in copies(n, 0):
                copy.wait()

    lanes = jnp.concatenate([y_ref[j] for j in range(y_ref.shape[0])], axis=1)
    acc = jnp.dot(lanes, w[step], preferred_element_type=F32)
    if which == 0:
        o_ref[...] = acc.astype(BF16)
    else:
        o_ref.reshape(rows, tile)[...] = (acc + add_ref[...].astype(F32)).astype(BF16)


def half_matmul(which, y, pieces, add=None):
    parts, rows, cols = y.shape
    width = pieces[0].shape[1]
    tile = 1024
    steps = width // tile
    if which == 0:
        out_spec = pl.BlockSpec((rows, tile), lambda n: (0, n))
        out_shape = jax.ShapeDtypeStruct((rows, width), BF16)
    else:
        out_spec = pl.BlockSpec((rows // 4, 4, tile), lambda n: (0, 0, n))
        out_shape = jax.ShapeDtypeStruct((rows // 4, 4, width), BF16)
    return pl.pallas_call(
        functools.partial(half_kernel, which),
        grid=(steps,),
        in_specs=[pl.BlockSpec(memory_space=pltpu.VMEM)]
        + [pl.BlockSpec(memory_space=pl.ANY)] * 8
        + ([pl.BlockSpec((rows, tile), lambda n: (0, n))] if which else []),
        out_specs=out_spec,
        out_shape=out_shape,
        scratch_shapes=[
            pltpu.VMEM((steps, parts * cols, tile), BF16),
            pltpu.SemaphoreType.DMA((steps, 16)),
        ],
        compiler_params=pltpu.CompilerParams(dimension_semantics=("arbitrary",)),
        cost_estimate=pl.CostEstimate(flops=512 * 2048 * 2048, transcendentals=0, bytes_accessed=8 << 20),
    )(pltpu.with_memory_space_constraint(y, pltpu.VMEM), *pieces, *([add] if which else []))


def ring_pairs(shift, first):
    pairs = []
    for z in range(4):
        for y in range(4):
            for t in range(8):
                along_y = (t % 2 == 0) == first
                to = (z, (y + shift) % 4) if along_y else ((z + shift) % 4, y)
                pairs.append(((z * 4 + y) * 8 + t, (to[0] * 4 + to[1]) * 8 + t))
    return pairs


def gather_line(half):
    both = ("sp", "tp")
    return [half] + [lax.ppermute(half, both, ring_pairs(k, True)) for k in (1, 2, 3)]


def gather_rest(line):
    both = ("sp", "tp")
    block = jnp.concatenate(line, axis=0)
    return [block] + [lax.ppermute(block, both, ring_pairs(k, False)) for k in (1, 2, 3)]


def with_partner(mine):
    swap = [(i, i ^ 1) for i in range(8)]
    return mine + [lax.ppermute(piece, "tp", swap) for piece in mine]


def body(
    inputs,
    norm_gain,
    pool_proj,
    pool_gate_proj,
    pool_mix,
    query_proj,
    key_proj,
    value_proj,
    attn_gate_proj,
    query_gain,
    key_gain,
    sink_logit,
    out_pool,
    out_attn,
):
    tp = lax.axis_index("tp")
    sp_size = lax.axis_size("sp")
    core = tp % 2
    half = jnp.where(core == 0, out_pool, out_attn)
    head, tail, w_pool, w_attn = first_rows(
        inputs, norm_gain[None, :], pool_proj, pool_gate_proj, query_proj, key_proj.T, value_proj.T, attn_gate_proj
    )
    up = [(i, i + 1) for i in range(sp_size - 1)]
    down = [(j, i) for i, j in up]
    half, head, tail = lax.optimization_barrier((half, head, tail))
    before = lax.ppermute(tail, "sp", up)
    after = lax.ppermute(head, "sp", down)
    line = gather_line(half)
    y_pool, scale = pool_branch(inputs, w_pool, pool_mix, before, after)
    *line, y_pool = lax.optimization_barrier((*line, y_pool))
    mine = gather_rest(line)
    pool_rows = lax.all_to_all(y_pool, "tp", split_axis=0, concat_axis=0, tiled=True)
    y_attn, lse = attn_branch(
        sink_logit, inputs, scale, w_attn, query_gain[None, :], key_gain[None, :], before, after
    )
    y_attn, pool_rows, *mine = lax.optimization_barrier((y_attn, pool_rows, *mine))
    pieces = with_partner(mine)
    attn_rows = lax.all_to_all(y_attn, "tp", split_axis=0, concat_axis=0, tiled=True)
    partial = half_matmul(0, pool_rows, pieces)
    mixed = half_matmul(1, attn_rows, pieces, partial)
    return mixed, jnp.transpose(lse, (2, 0, 1))


def solution(mesh):
    placed = (
        P("sp", None, None),
        P(),
        P(None, "tp"),
        P(None, "tp"),
        P("tp", None, None),
        P(None, "tp"),
        P(None, "tp"),
        P(None, "tp"),
        P(None, "tp"),
        P(),
        P(),
        P("tp"),
        P("sp", None),
        P("sp", None),
    )

    return jax.shard_map(
        body,
        mesh=mesh,
        in_specs=placed,
        out_specs=(P(("sp", "tp"), None, None), P("sp", None, "tp")),
        check_vma=False,
    )
```

```python
import functools
import math

import jax
import jax.numpy as jnp
from jax import lax
from jax.experimental import pallas as pl
from jax.experimental.pallas import tpu as pltpu
from jax.sharding import PartitionSpec as P


HEAD_DIM = 64
WINDOW = 128
REACH = 8
EPS = 1e-06
NEG = -1e30
LOG2E = math.log2(math.e)
F32 = jnp.float32
BF16 = jnp.bfloat16
BLOCK = 128


def row_scale(x):
    width = x.shape[1]
    acc = None
    for c in range(0, width, 128):
        part = x[:, c : c + 128].astype(F32)
        part = part * part
        acc = part if acc is None else acc + part
    total = jnp.sum(acc, axis=-1, keepdims=True)
    return lax.rsqrt(total * (1.0 / width) + EPS)


def silu(v):
    return v / (1.0 + jnp.exp(-v))


def first_kernel(
    x_ref, gain_ref, pool_ref, pgate_ref, query_ref, keyt_ref, valuet_ref, agate_ref,
    head_ref, tail_ref, wp_out, wa_out, w_edge, scr, xs, wp_ref, wa_ref, sems,
):
    half = x_ref.shape[0]
    step = pl.program_id(0)
    leave = [pltpu.make_async_copy(a, b, sems.at[n]) for n, (a, b) in enumerate(((wp_ref, wp_out), (wa_ref, wa_out)))]

    @pl.when(step == 0)
    def _():
        low = lax.broadcasted_iota(jnp.int32, (128, 128), 1) < HEAD_DIM
        for c in range(0, x_ref.shape[2], 128):
            rows = slice(c, c + 128)
            line = gain_ref[:, rows]
            column = jnp.broadcast_to(line, (128, 128)).T
            pool = (pool_ref[rows, :].astype(F32) * column).astype(BF16)
            wp_ref[rows, 0:128] = pool
            wp_ref[rows, 128:256] = (pgate_ref[rows, :].astype(F32) * column).astype(BF16)
            kv = (jnp.concatenate([keyt_ref[:, rows], valuet_ref[:, rows]], axis=0).astype(F32) * line).T
            turned = pltpu.roll(kv, HEAD_DIM, 1)
            wa_ref[rows, 0:128] = (query_ref[rows, :].astype(F32) * column).astype(BF16)
            wa_ref[rows, 128:256] = jnp.where(low, kv, turned).astype(BF16)
            wa_ref[rows, 256:384] = jnp.where(low, turned, kv).astype(BF16)
            wa_ref[rows, 384:512] = (agate_ref[rows, :].astype(F32) * column).astype(BF16)
            w_edge[rows, 0:128] = pool
            w_edge[rows, 128:256] = kv.astype(BF16)
        for copy in leave:
            copy.start()

    xs[...] = x_ref.reshape(half * 4, x_ref.shape[2])[...]
    x = xs[...]
    cols = jnp.dot(x, w_edge[...], preferred_element_type=F32) * row_scale(x)
    scr[0] = cols[:, :128]
    scr[1] = cols[:, 128:]
    for n in range(2):
        out = (head_ref, tail_ref)[n]

        @pl.when(step == n)
        def _(n=n, out=out):
            begin = n * 4 * (half - REACH)
            for s in range(4):
                out[s, 0:half, :] = scr[1, pl.ds(s, half, stride=4), :].astype(BF16)
                out[s, half : half + REACH, :] = scr[0, pl.ds(s + begin, REACH, stride=4), :].astype(BF16)

    @pl.when(step == 1)
    def _():
        for copy in leave:
            copy.wait()


def first_rows(x, gain, pool, pgate, query, keyt, valuet, agate):
    half = BLOCK
    width = x.shape[2]
    last = x.shape[0] // half
    whole = [gain, pool, pgate, query, keyt, valuet, agate]
    return pl.pallas_call(
        first_kernel,
        grid=(2,),
        in_specs=[pl.BlockSpec((half, 4, width), lambda i: (i * (last - 1), 0, 0))]
        + [pl.BlockSpec(a.shape, lambda i: (0, 0)) for a in whole],
        out_specs=(
            pl.BlockSpec((4, 136, 128), lambda i: (0, 0, 0)),
            pl.BlockSpec((4, 136, 128), lambda i: (0, 0, 0)),
            pl.BlockSpec(memory_space=pl.ANY),
            pl.BlockSpec(memory_space=pl.ANY),
        ),
        out_shape=(
            jax.ShapeDtypeStruct((4, 136, 128), BF16),
            jax.ShapeDtypeStruct((4, 136, 128), BF16),
            jax.ShapeDtypeStruct((width, 256), BF16),
            jax.ShapeDtypeStruct((width, 512), BF16),
        ),
        scratch_shapes=[
            pltpu.VMEM((width, 256), BF16),
            pltpu.VMEM((2, half * 4, 128), F32),
            pltpu.VMEM((half * 4, width), BF16),
            pltpu.VMEM((width, 256), BF16),
            pltpu.VMEM((width, 512), BF16),
            pltpu.SemaphoreType.DMA((2,)),
        ],
        compiler_params=pltpu.CompilerParams(dimension_semantics=("arbitrary",)),
        cost_estimate=pl.CostEstimate(flops=2 * 1024 * 2048 * 256, transcendentals=0, bytes_accessed=12 << 20),
        name="first_rows",
    )(x, *whole)


def pool_kernel(
    x_ref, w_hbm, mix_ref, before_ref, after_ref, y_hbm, scale_hbm, pool, gate, inverse, xs, xv, w_ref, yv, sv, sems, w_sem
):
    rows = BLOCK * 4
    blocks = xv.shape[0] // BLOCK
    pad = 64
    total_rows = blocks * rows
    power = lax.axis_index("tp") % 4
    half = jnp.left_shift(jnp.int32(1), power)

    def fetch(n):
        span = pl.ds(n * BLOCK, BLOCK)
        return pltpu.make_async_copy(x_ref.at[span], xv.at[span], sems.at[0, n])

    def leave(n):
        span = pl.ds(pl.multiple_of(n * rows, rows), rows)
        return (
            pltpu.make_async_copy(yv.at[n], y_hbm.at[n], sems.at[1, n]),
            pltpu.make_async_copy(sv.at[n], scale_hbm.at[span], sems.at[2, n]),
        )

    weights = pltpu.make_async_copy(w_hbm, w_ref, w_sem)
    weights.start()
    fetch(0).start()
    fetch(1).start()
    for s in range(4):
        pool[pl.ds(pad - 4 * REACH + s, REACH, stride=4), :] = before_ref[s, 128 : 128 + REACH, :].astype(F32)
        pool[pl.ds(pad + total_rows + s, REACH, stride=4), :] = after_ref[s, 128 : 128 + REACH, :].astype(F32)
    length = blocks * BLOCK
    begin = lax.axis_index("sp") * length
    total = lax.axis_size("sp") * length
    for k in range(3):
        where = (0, BLOCK, length - BLOCK)[k]
        position = begin + where + lax.broadcasted_iota(jnp.int32, (rows, 128), 0) // 4
        count = jnp.minimum(position + half - 1, total - 1) - jnp.maximum(position - half, 0) + 1
        inverse[k] = 1.0 / count.astype(F32)

    def finish(step):
        at = pl.multiple_of((step - 1) * rows, rows)
        base = pad + at
        reach = 4 * REACH
        window = pool[pl.ds(base - reach, rows + 2 * reach), :]
        size = rows + 2 * reach - 8
        two = window[:size] + window[4 : size + 4]
        four = two[: size - 8] + two[8:]
        eight = four[: size - 24] + four[16 : size - 8]
        sixteen = eight[: size - 56] + eight[32 : size - 24]
        sums = jnp.where(
            power == 0,
            two[reach - 4 : reach - 4 + rows],
            jnp.where(
                power == 1,
                four[reach - 8 : reach - 8 + rows],
                jnp.where(power == 2, eight[reach - 16 : reach - 16 + rows], sixteen[:rows]),
            ),
        )
        kind = jnp.where(step == 1, 0, jnp.where(step == blocks, 2, 1))
        pooled = (sums * inverse[kind] - window[reach : reach + rows]).astype(BF16)
        mixed = jnp.dot(pooled, mix_ref[0], preferred_element_type=F32)
        yv[step - 1] = (mixed * silu(gate[pl.ds(at, rows), :])).astype(BF16)
        for copy in leave(step - 1):
            copy.start()

    def project(step):
        fetch(step).wait()

        @pl.when(step + 2 < blocks)
        def _():
            fetch(step + 2).start()

        xs[...] = xv.at[pl.ds(pl.multiple_of(step * BLOCK, BLOCK), BLOCK)].reshape(rows, xv.shape[2])[...]
        x = xs[...]
        scale = row_scale(x)
        sv[step] = jnp.broadcast_to(scale, (rows, 128))
        both = jnp.dot(x, w_ref[...], preferred_element_type=F32) * scale
        at = pl.multiple_of(step * rows, rows)
        pool[pl.ds(pad + at, rows), :] = both[:, :128]
        gate[pl.ds(at, rows), :] = both[:, 128:]

    weights.wait()
    project(0)

    @pl.loop(1, blocks)
    def _(step):
        project(step)
        finish(step)

    finish(blocks)
    for n in range(blocks):
        for copy in leave(n):
            copy.wait()


def pool_branch(x, w, mix, before, after):
    length, _, width = x.shape
    blocks = length // BLOCK
    rows = BLOCK * 4
    whole = pl.BlockSpec(memory_space=pltpu.VMEM)
    far = pl.BlockSpec(memory_space=pl.ANY)
    return pl.pallas_call(
        pool_kernel,
        in_specs=[far, far, whole, whole, whole],
        out_specs=(far, far),
        out_shape=(
            jax.ShapeDtypeStruct((blocks, rows, 128), BF16),
            jax.ShapeDtypeStruct((length * 4, 128), F32),
        ),
        scratch_shapes=[
            pltpu.VMEM((length * 4 + 128, 128), F32),
            pltpu.VMEM((length * 4, 128), F32),
            pltpu.VMEM((3, rows, 128), F32),
            pltpu.VMEM((rows, width), BF16),
            pltpu.VMEM(x.shape, BF16),
            pltpu.VMEM(w.shape, BF16),
            pltpu.VMEM((blocks, rows, 128), BF16),
            pltpu.VMEM((blocks, rows, 128), F32),
            pltpu.SemaphoreType.DMA((3, blocks)),
            pltpu.SemaphoreType.DMA,
        ],
        cost_estimate=pl.CostEstimate(flops=2 * 4096 * 2048 * 256, transcendentals=0, bytes_accessed=18 << 20),
        name="pool_branch",
    )(x, w, mix, before, after)


def attn_kernel(
    sink_ref, x_ref, scale_ref, w_ref, qgain_ref, kgain_ref, before_ref, after_ref,
    y_ref, lse_ref, proj, qs, ks, vs, gate, bias, att, xs, sinks, gains, same,
):
    step = pl.program_id(0)
    blocks = pl.num_programs(0) - 1
    rows = BLOCK * 4
    lane = lax.broadcasted_iota(jnp.int32, (BLOCK, 128), 1)
    low_lanes = lane < HEAD_DIM
    shifts = [jnp.maximum(sink_ref[h], 0.0) for h in range(2)]

    @pl.when(step == 0)
    def _():
        query = lax.broadcasted_iota(jnp.int32, (BLOCK, 3 * BLOCK), 0)
        key = lax.broadcasted_iota(jnp.int32, (BLOCK, 3 * BLOCK), 1) - BLOCK
        distance = jnp.abs(query - key)
        r = lax.broadcasted_iota(jnp.int32, (256, 256), 0) // HEAD_DIM
        c = lax.broadcasted_iota(jnp.int32, (256, 256), 1) // HEAD_DIM
        same[...] = jnp.where(r == c, 1.0, 0.0).astype(BF16)
        scale = lax.broadcasted_iota(jnp.int32, (BLOCK, 3 * BLOCK), 0) * 0 + jnp.left_shift(
            jnp.int32(1), lax.axis_index("tp")
        )
        for h in range(2):
            slope = ((0.5**0.5, 0.5)[h] * LOG2E) / scale.astype(F32)
            line = -slope * distance.astype(F32) - shifts[h] * LOG2E
            bias[h * BLOCK : (h + 1) * BLOCK, :] = jnp.where(distance <= WINDOW, line, NEG)
        shift_row = jnp.where(low_lanes, shifts[0], shifts[1])
        sink_row = jnp.where(low_lanes, sink_ref[0], sink_ref[1])
        sinks[...] = jnp.exp(sink_row - shift_row)
        qgain = qgain_ref[...] * (LOG2E * HEAD_DIM**-0.5)
        gains[...] = jnp.concatenate([qgain, qgain, kgain_ref[...], kgain_ref[...]], axis=1)
        key_gain = jnp.concatenate([kgain_ref[...], kgain_ref[...]], axis=1)
        sp = lax.axis_index("sp")
        for side, ref in enumerate((before_ref, after_ref)):
            at = 0 if side == 0 else (blocks + 1) * BLOCK
            live = (sp > 0) if side == 0 else (sp < lax.axis_size("sp") - 1)
            live = jnp.where(live, 1.0, 0.0)
            for s in range(4):
                kv = ref[s, 0:128, :].astype(F32)
                turned = pltpu.roll(kv, HEAD_DIM, 1)
                kk = jnp.where(low_lanes, kv, turned)
                vv = jnp.where(low_lanes, turned, kv)
                mean = jnp.sum(jnp.where(low_lanes, kv * kv, 0.0), axis=-1, keepdims=True) * (1.0 / HEAD_DIM)
                ks[s, pl.ds(at, BLOCK), :] = (kk * lax.rsqrt(mean + EPS) * key_gain).astype(BF16)
                vs[s, pl.ds(at, BLOCK), 0:128] = vv.astype(BF16)
                vs[s, pl.ds(at, BLOCK), 128:256] = jnp.full((BLOCK, 128), live, F32).astype(BF16)

    def project():
        size, at = rows, 0
        xs[...] = x_ref.reshape(rows, x_ref.shape[2])[...]
        x = xs[...]
        cols = jnp.dot(x, w_ref[...], preferred_element_type=F32)
        scale = scale_ref[at : at + size, :]
        qk = cols[:, :256] * jnp.concatenate([scale, scale], axis=1)
        squares = jnp.dot((qk * qk).astype(BF16), same[...], preferred_element_type=F32)
        normed = qk * lax.rsqrt(squares * (1.0 / HEAD_DIM) + EPS) * gains[...]
        proj[0, at : at + size] = normed[:, :128]
        proj[1, at : at + size] = normed[:, 128:]
        proj[2, at : at + size] = cols[:, 256:384] * scale
        gate[step % 2, at : at + size, :] = cols[:, 384:] * scale

    def separate():
        at = pl.multiple_of(step * BLOCK, BLOCK)
        for s in range(4):
            mine = pl.ds(s, BLOCK, stride=4)
            qs[step % 2, s] = proj[0, mine, :].astype(BF16)
            ks[s, pl.ds(at + BLOCK, BLOCK), :] = proj[1, mine, :].astype(BF16)
            vs[s, pl.ds(at + BLOCK, BLOCK), 0:128] = proj[2, mine, :].astype(BF16)
            vs[s, pl.ds(at + BLOCK, BLOCK), 128:256] = jnp.ones((BLOCK, 128), BF16)

    def attend(s):
        at = pl.multiple_of((step - 1) * BLOCK, BLOCK)
        q = qs[(step - 1) % 2, s]
        zero = jnp.zeros_like(q)
        two = jnp.concatenate([jnp.where(low_lanes, q, zero), jnp.where(low_lanes, zero, q)], axis=0)
        keys = ks[s, pl.ds(at, 3 * BLOCK), :]
        score = lax.dot_general(two, keys, (((1,), (1,)), ((), ())), preferred_element_type=F32)
        weight = jnp.exp2(score + bias[...]).astype(BF16)
        out = jnp.dot(weight, vs[s, pl.ds(at, 3 * BLOCK), :], preferred_element_type=F32)
        total = jnp.where(low_lanes, out[:BLOCK, 128:], out[BLOCK:, 128:]) + sinks[...]
        value = jnp.where(low_lanes, out[:BLOCK, :128], out[BLOCK:, :128])
        att[pl.ds(s, BLOCK, stride=4), :] = value / total
        turned = total.T
        lse_ref[s, 0:1, :] = jnp.log(turned[0:1, :]) + shifts[0]
        lse_ref[s, 1:2, :] = jnp.log(turned[HEAD_DIM : HEAD_DIM + 1, :]) + shifts[1]

    def close():
        y_ref[0] = (att[...] * silu(gate[(step - 1) % 2])).astype(BF16)

    @pl.when(step < blocks)
    def _():
        project()
        separate()

    @pl.when(step > 0)
    def _():
        for s in range(4):
            attend(s)
        close()


def attn_branch(sink, x, scale, w, qgain, kgain, before, after):
    length, _, width = x.shape
    blocks = length // BLOCK
    rows = BLOCK * 4
    return pl.pallas_call(
        attn_kernel,
        grid=(blocks + 1,),
        in_specs=[
            pl.BlockSpec(memory_space=pltpu.SMEM),
            pl.BlockSpec((BLOCK, 4, width), lambda i: (jnp.minimum(i, blocks - 1), 0, 0)),
            pl.BlockSpec((rows, 128), lambda i: (jnp.minimum(i, blocks - 1), 0)),
            pl.BlockSpec(w.shape, lambda i: (0, 0)),
            pl.BlockSpec(qgain.shape, lambda i: (0, 0)),
            pl.BlockSpec(kgain.shape, lambda i: (0, 0)),
            pl.BlockSpec(before.shape, lambda i: (0, 0, 0)),
            pl.BlockSpec(after.shape, lambda i: (0, 0, 0)),
        ],
        out_specs=(
            pl.BlockSpec((1, rows, 128), lambda i: (jnp.maximum(i - 1, 0), 0, 0)),
            pl.BlockSpec((4, 2, BLOCK), lambda i: (0, 0, jnp.maximum(i - 1, 0))),
        ),
        out_shape=(
            jax.ShapeDtypeStruct((blocks, rows, 128), BF16),
            jax.ShapeDtypeStruct((4, 2, length), F32),
        ),
        scratch_shapes=[
            pltpu.VMEM((3, rows, 128), F32),
            pltpu.VMEM((2, 4, BLOCK, 128), BF16),
            pltpu.VMEM((4, length + 2 * BLOCK, 128), BF16),
            pltpu.VMEM((4, length + 2 * BLOCK, 256), BF16),
            pltpu.VMEM((2, rows, 128), F32),
            pltpu.VMEM((2 * BLOCK, 3 * BLOCK), F32),
            pltpu.VMEM((rows, 128), F32),
            pltpu.VMEM((rows, width), BF16),
            pltpu.VMEM((BLOCK, 128), F32),
            pltpu.VMEM((1, 256), F32),
            pltpu.VMEM((256, 256), BF16),
        ],
        compiler_params=pltpu.CompilerParams(dimension_semantics=("arbitrary",)),
        cost_estimate=pl.CostEstimate(flops=2 * 4096 * 2048 * 768, transcendentals=3 << 20, bytes_accessed=20 << 20),
        name="attn_branch",
    )(sink, x, scale, w, qgain, kgain, before, after)


def half_kernel(which, y_ref, *rest):
    pieces, rest = rest[:8], rest[8:]
    add_ref, (o_ref, w, sems) = (None, rest) if which == 0 else (rest[0], rest[1:])
    tiles, _, tile = w.shape
    rows = y_ref.shape[1]
    step = pl.program_id(0)
    place = lax.axis_index("sp")
    z, y, core = place // 4, place % 4, lax.axis_index("tp") % 2

    def copies(n, side):
        for m in range(4):
            for k in range(4):
                a = (z + 4 - (m if which == 0 else k)) % 4
                b = (y + 4 - (k if which == 0 else m)) % 4
                row = pl.multiple_of((a * 4 + b) * 64, 64)
                yield pltpu.make_async_copy(
                    pieces[side * 4 + m].at[pl.ds(k * 64, 64), pl.ds(n * tile, tile)],
                    w.at[n, pl.ds(row, 64), :],
                    sems.at[n, m * 4 + k],
                )

    for side in range(2):

        @pl.when((step == 0) & (core == (which if side == 0 else 1 - which)))
        def _(side=side):
            for n in range(tiles):
                for copy in copies(n, side):
                    copy.start()

    for n in range(tiles):

        @pl.when(step == n)
        def _(n=n):
            for copy in copies(n, 0):
                copy.wait()

    lanes = jnp.concatenate([y_ref[j] for j in range(y_ref.shape[0])], axis=1)
    acc = jnp.dot(lanes, w[step], preferred_element_type=F32)
    if which == 0:
        o_ref[...] = acc.astype(BF16)
    else:
        o_ref.reshape(rows, tile)[...] = (acc + add_ref[...].astype(F32)).astype(BF16)


def half_matmul(which, y, pieces, add=None):
    parts, rows, cols = y.shape
    width = pieces[0].shape[1]
    tile = 1024
    steps = width // tile
    if which == 0:
        out_spec = pl.BlockSpec((rows, tile), lambda n: (0, n))
        out_shape = jax.ShapeDtypeStruct((rows, width), BF16)
    else:
        out_spec = pl.BlockSpec((rows // 4, 4, tile), lambda n: (0, 0, n))
        out_shape = jax.ShapeDtypeStruct((rows // 4, 4, width), BF16)
    return pl.pallas_call(
        functools.partial(half_kernel, which),
        grid=(steps,),
        in_specs=[pl.BlockSpec(memory_space=pltpu.VMEM)]
        + [pl.BlockSpec(memory_space=pl.ANY)] * 8
        + ([pl.BlockSpec((rows, tile), lambda n: (0, n))] if which else []),
        out_specs=out_spec,
        out_shape=out_shape,
        scratch_shapes=[
            pltpu.VMEM((steps, parts * cols, tile), BF16),
            pltpu.SemaphoreType.DMA((steps, 16)),
        ],
        compiler_params=pltpu.CompilerParams(dimension_semantics=("arbitrary",)),
        cost_estimate=pl.CostEstimate(flops=512 * 2048 * 2048, transcendentals=0, bytes_accessed=8 << 20),
    )(pltpu.with_memory_space_constraint(y, pltpu.VMEM), *pieces, *([add] if which else []))


def ring_pairs(shift, first):
    pairs = []
    for z in range(4):
        for y in range(4):
            for t in range(8):
                along_y = (t % 2 == 0) == first
                to = (z, (y + shift) % 4) if along_y else ((z + shift) % 4, y)
                pairs.append(((z * 4 + y) * 8 + t, (to[0] * 4 + to[1]) * 8 + t))
    return pairs


def gather_line(half):
    both = ("sp", "tp")
    return [half] + [lax.ppermute(half, both, ring_pairs(k, True)) for k in (1, 2, 3)]


def gather_rest(line):
    both = ("sp", "tp")
    block = jnp.concatenate(line, axis=0)
    return [block] + [lax.ppermute(block, both, ring_pairs(k, False)) for k in (1, 2, 3)]


def with_partner(mine):
    swap = [(i, i ^ 1) for i in range(8)]
    return mine + [lax.ppermute(piece, "tp", swap) for piece in mine]


def body(
    inputs,
    norm_gain,
    pool_proj,
    pool_gate_proj,
    pool_mix,
    query_proj,
    key_proj,
    value_proj,
    attn_gate_proj,
    query_gain,
    key_gain,
    sink_logit,
    out_pool,
    out_attn,
):
    tp = lax.axis_index("tp")
    sp_size = lax.axis_size("sp")
    core = tp % 2
    half = jnp.where(core == 0, out_pool, out_attn)
    head, tail, w_pool, w_attn = first_rows(
        inputs, norm_gain[None, :], pool_proj, pool_gate_proj, query_proj, key_proj.T, value_proj.T, attn_gate_proj
    )
    up = [(i, i + 1) for i in range(sp_size - 1)]
    down = [(j, i) for i, j in up]
    half, head, tail = lax.optimization_barrier((half, head, tail))
    before = lax.ppermute(tail, "sp", up)
    after = lax.ppermute(head, "sp", down)
    line = gather_line(half)
    y_pool, scale = pool_branch(inputs, w_pool, pool_mix, before, after)
    *line, y_pool = lax.optimization_barrier((*line, y_pool))
    mine = gather_rest(line)
    pool_rows = lax.all_to_all(y_pool, "tp", split_axis=0, concat_axis=0, tiled=True)
    y_attn, lse = attn_branch(
        sink_logit, inputs, scale, w_attn, query_gain[None, :], key_gain[None, :], before, after
    )
    y_attn, pool_rows, *mine = lax.optimization_barrier((y_attn, pool_rows, *mine))
    pieces = [pltpu.with_memory_space_constraint(piece, pltpu.HBM) for piece in with_partner(mine)]
    attn_rows = lax.all_to_all(y_attn, "tp", split_axis=0, concat_axis=0, tiled=True)
    partial = half_matmul(0, pool_rows, pieces)
    mixed = half_matmul(1, attn_rows, pieces, partial)
    return mixed, jnp.transpose(lse, (2, 0, 1))


def solution(mesh):
    placed = (
        P("sp", None, None),
        P(),
        P(None, "tp"),
        P(None, "tp"),
        P("tp", None, None),
        P(None, "tp"),
        P(None, "tp"),
        P(None, "tp"),
        P(None, "tp"),
        P(),
        P(),
        P("tp"),
        P("sp", None),
        P("sp", None),
    )

    return jax.shard_map(
        body,
        mesh=mesh,
        in_specs=placed,
        out_specs=(P(("sp", "tp"), None, None), P("sp", None, "tp")),
        check_vma=False,
    )
```
